32 devices in a mesh: sp: 8 (over z, core), tp: 4 (over y, x).
Axes of the slice: x: 2, y: 2, z: 4, core: 2. Of those that a mesh axis runs over, the one named last changes fastest.
Arguments:
- residual_in: bfloat16 [1024, 2048], P('sp'), may hold values from -6 to 6
- queries: bfloat16 [1024, 2048], P('sp', 'tp'), may hold values from -6 to 6
- keys: bfloat16 [1024, 2048], P('sp', 'tp'), may hold values from -6 to 6
- values: bfloat16 [1024, 2048], P('sp', 'tp'), may hold values from -6 to 6
- out_gate: bfloat16 [1024, 2048], P('sp', 'tp'), may hold values from -6 to 6
- beta_logit: bfloat16 [16, 1024], P('tp', 'sp'), may hold values from -6 to -2
- decay_logit: bfloat16 [16, 1024], P('tp', 'sp'), may hold values from -4.5 to 4.5
- decay_log: float32 [16], P('tp'), may hold values from -11 to -3.2
- head_gain: float32 [128], replicated, may hold values from 0.1 to 1.9
- out_weight: bfloat16 [2048, 2048], P('tp'), may hold values from -0.125 to 0.125
- norm_gain: float32 [2048], replicated, may hold values from 0.1 to 1.9
- final_gain: float32 [2048], replicated, may hold values from 0.1 to 1.9
- expert_index: int32 [1024, 2], P('sp'), may hold values from 0 to 7, all different within a row; in each aligned block of 32 rows (0 to 31, 32 to 63, ...) at most 16 rows name the same one
- route_weights: float32 [1024, 2], P('sp'), may hold values from 0.2 to 1
- expert_gate: bfloat16 [8, 2048, 6144], P('sp', None, 'tp'), may hold values from -0.125 to 0.125
- expert_up: bfloat16 [8, 2048, 6144], P('sp', None, 'tp'), may hold values from -0.125 to 0.125
- expert_down: bfloat16 [8, 6144, 2048], P('sp', 'tp'), may hold values from -0.078125 to 0.078125
Outputs:
- layer_out: bfloat16 [1024, 2048], P('sp')
The draws below stay inside these ranges and needn't reach their ends.
Inputs may be any that keep to these rules, and one draw needn't show every extreme that they name: `expert_index`: in each aligned block of 32 rows no expert is named by more than 16 rows, a bound that some block reaches; a row names 2 different experts.
All inputs are finite; a program needn't handle non-finite values.
Results may differ from the reference program's by a relative error of at most 0.015.
Values may be sent and summed in bfloat16 or wider, within the bound.
A program may use at most 64 MiB of HBM per device.

```python
import math
import jax
import jax.numpy as jnp
import numpy as np
from jax import lax

D = 2048
HEADS = 16
HEAD_FEATURES = 128
FF = 6144
TOP = 2
BLOCK = 64
TOKENS = 1024
EXPERTS = 8
ROWS_TP = 32
CAP = 16
N_SP = 8
N_TP = 4


def draw_decay_logit(key, part):
    noise_key, level_key = jax.random.split(key)
    noise = jax.random.truncated_normal(noise_key, -3.0, 3.0, (HEADS, TOKENS), jnp.float32)
    levels = jax.random.uniform(level_key, (HEADS, TOKENS // 128), jnp.float32, -1.5, 1.5)
    return (noise + jnp.repeat(levels, 128, axis=1)).astype(jnp.bfloat16)


def draw_decay_log(key, part):
    pick_key, slow_key, fast_key = jax.random.split(key, 3)
    share = 0.5
    slow = jax.random.uniform(pick_key, (HEADS,), jnp.float32) < share
    slow_value = jax.random.uniform(slow_key, (HEADS,), jnp.float32, -11.0, -9.5)
    fast_value = jax.random.uniform(fast_key, (HEADS,), jnp.float32, -4.2, -3.2)
    return jnp.where(slow, slow_value, fast_value)


def steps_of(own_key, dims, cuts, smallest, top_value):
    def one(position, shards_of):
        steps = jax.random.uniform(jax.random.fold_in(jax.random.fold_in(own_key, 6), position), (shards_of,), jnp.float32, smallest / len(cuts), top_value / len(cuts))
        return jnp.repeat(jnp.exp(steps), dims[position] // shards_of).reshape((-1,) + (1,) * (len(dims) - position - 1))

    factor_of = one(*cuts[0])
    for cut in cuts[1:]:
        factor_of = factor_of * one(*cut)
    return factor_of


def deal_out(rng, own, number, rows, number_of, top, reach, slope):
    sequence = jax.random.permutation(rng, number_of)
    crowded, ordinary = shares(number_of, rows * top, reach, slope, True), shares(number_of, rows * top, reach, slope, False)
    places = jnp.arange(number_of)

    def named(sizes, turn):
        used = int((sizes > 0).sum())
        fixed = max(1, used // 4)
        shifted = fixed + (places - fixed + turn * (used - fixed)) % max(1, number_of - fixed)
        return jnp.zeros((number_of,), jnp.int32).at[sequence[jnp.where(places < fixed, places, shifted)]].set(jnp.asarray(sizes, jnp.int32))

    sizes = jnp.where(number % 4 == 0, named(crowded, number // 4), named(ordinary, number - number // 4 - 1))
    mixed = jax.random.permutation(jax.random.fold_in(own, 3), number_of)
    donor, receiver = mixed[0:number_of // 2 * 2:2], mixed[1:number_of // 2 * 2:2]
    room = jnp.minimum(sizes[donor] - 1, reach - sizes[receiver]) // 2
    room = jnp.where((donor == sequence[0]) | (receiver == sequence[0]) | (sizes[receiver] == 0), 0, jnp.maximum(room, 0))
    shifted = jax.random.randint(jax.random.fold_in(own, 4), (number_of // 2,), 0, 1 << 20) % (room + 1)
    sizes = sizes.at[donor].add(-shifted).at[receiver].add(shifted)
    items = jnp.searchsorted(jnp.cumsum(sizes), jnp.arange(rows * top), side="right").astype(jnp.int32)
    table = items.reshape(top, rows).T
    table = table[jax.random.permutation(jax.random.fold_in(own, 1), rows)]
    turn = jax.random.randint(jax.random.fold_in(own, 2), (rows, 1), 0, top)
    return jnp.take_along_axis(table, (jnp.arange(top)[None, :] + turn) % top, axis=1)


def shares(count, total, bound, slope, full):
    weights = [(1 << 20) // math.isqrt(standing ** slope) + 1 for standing in range(1, count + 1)]
    largest = bound if full else min(bound, max(-(-total // count), total * weights[0] // sum(weights)))
    least = 1 if total - largest >= count - 1 else 0
    holding, surplus = [largest] + [least] * (count - 1), total - largest - least * (count - 1)
    while surplus > 0:
        candidates = [i for i in range(1, count) if holding[i] < largest] or [i for i in range(1, count) if holding[i] < bound]
        whole, budget = sum([weights[i] for i in candidates]), surplus
        for i in candidates:
            extra = min(bound - holding[i], max(1, budget * weights[i] // whole), surplus)
            holding[i] = holding[i] + extra
            surplus = surplus - extra
    return np.array(holding)


def scatter_about(rng, shape, scale, reach, pieces=(), kind=jnp.bfloat16):
    array = jax.random.normal(rng, shape, jnp.float32) * scale
    if len(pieces) > 0:
        array = steps_of(rng, shape, pieces, -0.22, 0.18) * array
    return jnp.clip(array, min=-reach, max=reach).astype(kind)


def setup_inputs(seed: int = 0) -> dict:
    splits = jax.random.split(jax.random.key(seed), 18)
    residual_in = scatter_about(splits[0], (TOKENS, D), 1.0, 6.0, ((0, 8),))
    queries = scatter_about(splits[1], (TOKENS, HEADS * HEAD_FEATURES), 1.0, 6.0, ((0, 8), (1, 4)))
    keys = scatter_about(splits[2], (TOKENS, HEADS * HEAD_FEATURES), 1.0, 6.0, ((0, 8), (1, 4)))
    values = scatter_about(splits[3], (TOKENS, HEADS * HEAD_FEATURES), 1.0, 6.0, ((0, 8), (1, 4)))
    out_gate = scatter_about(splits[4], (TOKENS, HEADS * HEAD_FEATURES), 1.0, 6.0, ((0, 8), (1, 4)))
    beta_logit = jnp.clip(-6.0 + 4.0 * jax.random.uniform(splits[5], (HEADS, TOKENS), jnp.float32) ** steps_of(splits[5], (HEADS, TOKENS), ((0, 4), (1, 8)), -0.2, 0.2), -6.0, -2.0).astype(jnp.bfloat16)
    decay_logit = draw_decay_logit(jax.random.fold_in(splits[17], 71), 0)
    decay_log = draw_decay_log(jax.random.fold_in(splits[17], 71), 0)
    head_gain = jnp.clip(1.0 + 0.18 * jax.random.normal(splits[8], (HEAD_FEATURES,), jnp.float32), 0.1, 1.9)
    out_weight = scatter_about(splits[9], (HEADS * HEAD_FEATURES, D), (HEADS * HEAD_FEATURES) ** -0.5, 0.125, ((0, 4),))
    norm_gain = jnp.clip(1.0 + 0.18 * jax.random.normal(splits[10], (D,), jnp.float32), 0.1, 1.9)
    final_gain = jnp.clip(1.0 + 0.18 * jax.random.normal(splits[11], (D,), jnp.float32), 0.1, 1.9)
    expert_index_keys = jax.random.split(jax.random.fold_in(splits[12], 1), TOKENS // ROWS_TP)
    expert_index_turns = jax.random.permutation(jax.random.fold_in(splits[12], 3), TOKENS // ROWS_TP)
    expert_index = jax.vmap(lambda own, number: deal_out(jax.random.fold_in(splits[12], 2), own, number, ROWS_TP, EXPERTS, TOP, CAP, 1))(expert_index_keys, expert_index_turns).reshape((TOKENS, TOP))
    route_weights = jnp.clip(0.2 + 0.8 * jax.random.uniform(splits[13], (TOKENS, TOP), jnp.float32) ** steps_of(splits[13], (TOKENS, TOP), ((0, 8),), -0.2, 0.2), 0.2, 1.0)
    expert_gate = scatter_about(splits[14], (EXPERTS, D, FF), D ** -0.5, 0.125, ((0, 8), (2, 4)))
    expert_up = scatter_about(splits[15], (EXPERTS, D, FF), D ** -0.5, 0.125, ((0, 8), (2, 4)))
    expert_down = scatter_about(splits[16], (EXPERTS, FF, D), FF ** -0.5, 0.078125, ((0, 8), (1, 4)))
    return dict(residual_in=residual_in, queries=queries, keys=keys, values=values, out_gate=out_gate, beta_logit=beta_logit, decay_logit=decay_logit, decay_log=decay_log, head_gain=head_gain, out_weight=out_weight, norm_gain=norm_gain, final_gain=final_gain, expert_index=expert_index, route_weights=route_weights, expert_gate=expert_gate, expert_up=expert_up, expert_down=expert_down)


highest_precision = lax.Precision.HIGHEST
residual_scale = 2.0 ** 0.5

def unit_rows(data):
    return data * lax.rsqrt(lax.optimization_barrier(jnp.sum(data * data, -1, keepdims=True)) + 1e-06)

def layer_norm(data, gain):
    center = data - lax.optimization_barrier(jnp.mean(data, -1, keepdims=True))
    return center * lax.rsqrt(lax.optimization_barrier(jnp.mean(center * center, -1, keepdims=True)) + 1e-05) * gain

def rounded(data):
    return lax.optimization_barrier(data.astype(jnp.bfloat16)).astype(jnp.float32)

def delta_blocks(query, key, value, beta, decay):
    heads, length, width = query.shape
    count = length // BLOCK
    shape = (heads, count, BLOCK, width)
    query = query.reshape(shape)
    key = key.reshape(shape)
    value = value.reshape(shape)
    beta = beta.reshape(heads, count, BLOCK)
    running = jnp.cumsum(decay.reshape(heads, count, BLOCK), axis=-1)
    causal = jnp.tril(jnp.ones((BLOCK, BLOCK), bool))
    strict = jnp.tril(jnp.ones((BLOCK, BLOCK), bool), -1)
    within = jnp.exp(jnp.where(causal, running[..., :, None] - running[..., None, :], -jnp.inf))
    key_beta = key * beta[..., None]
    lower = jnp.where(strict, jnp.einsum('hnid,hnjd->hnij', key_beta, key, precision=highest_precision) * within, 0.0)
    system = jnp.eye(BLOCK, dtype=jnp.float32) + lower
    fresh = jax.scipy.linalg.solve_triangular(system, value * beta[..., None], lower=True, unit_diagonal=True)
    weighted = jax.scipy.linalg.solve_triangular(system, key_beta * jnp.exp(running)[..., None], lower=True, unit_diagonal=True)
    scores = jnp.einsum('hnid,hnjd->hnij', query, key, precision=highest_precision) * within
    query_decayed = query * jnp.exp(running)[..., None]
    key_decayed = key * jnp.exp(running[..., -1:] - running)[..., None]
    block_decay = jnp.exp(running[..., -1])

    def advance(recurrent_state, inputs):
        fresh_value_block, block_weighted_values, block_queries, block_keys, block_scores, block_decay_factor = inputs
        corrected_value = fresh_value_block - jnp.einsum('nya,nag->nyg', block_weighted_values, recurrent_state, precision=highest_precision)
        final_output = jnp.einsum('nya,nag->nyg', block_queries, recurrent_state, precision=highest_precision) + jnp.einsum('emp,epk->emk', block_scores, corrected_value, precision=highest_precision)
        recurrent_state = block_decay_factor[:, None, None] * recurrent_state + jnp.einsum('iyp,iyu->ipu', block_keys, corrected_value, precision=highest_precision)
        return (recurrent_state, final_output)
    start = jnp.zeros((heads, width, width), jnp.float32)
    inputs = tuple((jnp.moveaxis(item, 1, 0) for item in (fresh, weighted, query_decayed, key_decayed, scores, block_decay)))
    _, output_list = lax.scan(advance, start, inputs)
    return jnp.moveaxis(output_list, 0, 1).reshape(heads, length, width)

def reference(residual_in, queries, keys, values, out_gate, beta_logit, decay_logit, decay_log, head_gain, out_weight, norm_gain, final_gain, expert_index, route_weights, expert_gate, expert_up, expert_down):
    length, width = residual_in.shape
    heads = beta_logit.shape[0]

    def split_heads(data):
        return data.astype(jnp.float32).reshape(length, heads, HEAD_FEATURES).transpose(1, 0, 2)
    query = unit_rows(split_heads(queries)) * HEAD_FEATURES ** (-0.5)
    key = unit_rows(split_heads(keys))
    value = split_heads(values)
    beta = jax.nn.sigmoid(beta_logit.astype(jnp.float32))
    decay = -jnp.exp(decay_log)[:, None] * jax.nn.softplus(decay_logit.astype(jnp.float32))
    mixed = delta_blocks(query, key, value, beta, decay)
    normalized = mixed * lax.rsqrt(lax.optimization_barrier(jnp.mean(mixed * mixed, -1, keepdims=True)) + 1e-06) * head_gain
    gated = (normalized * jax.nn.silu(split_heads(out_gate))).transpose(1, 0, 2).reshape(length, heads * HEAD_FEATURES).astype(jnp.bfloat16)
    group = heads * HEAD_FEATURES // N_TP
    projected = jnp.zeros((length, width), jnp.float32)
    for index in range(N_TP):
        projected = projected + rounded(jnp.dot(gated[:, index * group:(index + 1) * group].astype(jnp.float32), out_weight[index * group:(index + 1) * group].astype(jnp.float32), preferred_element_type=jnp.float32))
    hidden_in = layer_norm(residual_scale * residual_in.astype(jnp.float32) + projected, norm_gain).astype(jnp.bfloat16)
    total = length * TOP
    flat = expert_index.reshape(total).astype(jnp.int32)
    largest = N_SP * N_TP * CAP
    slice_width = FF // N_TP

    def one_expert(inputs):
        index, gate_matrix, up_matrix, down_matrix = inputs
        positions = jnp.nonzero(flat == index, size=largest, fill_value=total)[0].astype(jnp.int32)
        rows = hidden_in[jnp.minimum(positions, total - 1) // TOP]
        gate = jnp.dot(rows.astype(jnp.float32), gate_matrix.astype(jnp.float32), preferred_element_type=jnp.float32)
        up = jnp.dot(rows.astype(jnp.float32), up_matrix.astype(jnp.float32), preferred_element_type=jnp.float32)
        inner = (jax.nn.silu(gate) * up).astype(jnp.bfloat16)
        summed = jnp.zeros((largest, width), jnp.float32)
        for part in range(N_TP):
            summed = summed + rounded(jnp.dot(inner[:, part * slice_width:(part + 1) * slice_width].astype(jnp.float32), down_matrix[part * slice_width:(part + 1) * slice_width].astype(jnp.float32), preferred_element_type=jnp.float32))
        return (summed.astype(jnp.bfloat16), positions)
    output_list, positions = lax.map(one_expert, (jnp.arange(EXPERTS, dtype=jnp.int32), expert_gate, expert_up, expert_down))
    placed = jnp.zeros((total + 1, width), jnp.bfloat16).at[positions.reshape(-1)].set(output_list.reshape(-1, width))
    chosen = placed[:total].reshape(length, TOP, width).astype(jnp.float32)
    routed = lax.optimization_barrier(jnp.sum(route_weights[..., None] * chosen, 1))
    return layer_norm(residual_scale * hidden_in.astype(jnp.float32) + routed, final_gain).astype(jnp.bfloat16)
```

```python
import functools

import jax
import jax.numpy as jnp
from jax import lax
from jax.experimental import pallas as pl
from jax.experimental.pallas import tpu as pltpu
from jax.sharding import PartitionSpec as P

MESH = pl.DeviceIdType.MESH

HEAD_FEATURES = 128
TOP = 2
BLOCK = 64
GROUP = 2


highest_precision = lax.Precision.HIGHEST
residual_scale = 2.0**0.5


def carried_in(x, axis, join, neutral):
    place = lax.axis_index(axis)
    gathered = jax.tree.map(
        lambda a, kind: lax.all_gather(a.astype(kind), axis), x, (jnp.bfloat16, jnp.bfloat16)
    )
    state = jax.tree.map(lambda a, e: jnp.zeros_like(a) + jnp.asarray(e, a.dtype), x, neutral)

    def one(turn, state):
        return join(
            state,
            jax.tree.map(
                lambda a, own: lax.dynamic_index_in_dim(a, turn, 0, False).astype(own.dtype),
                gathered,
                x,
            ),
        )

    return lax.fori_loop(0, place, one, state)


def unit_rows(data):
    return data * lax.rsqrt(jnp.sum(data * data, -1, keepdims=True) + 1e-06)


def layer_norm(data, gain):
    center = data - jnp.mean(data, -1, keepdims=True)
    return center * lax.rsqrt(jnp.mean(center * center, -1, keepdims=True) + 1e-05) * gain


def block_terms(query, key, beta, decay):
    heads, length, width = query.shape
    count = length // BLOCK
    shape = (heads, count, BLOCK, width)
    query = query.reshape(shape)
    key = key.reshape(shape)
    beta = beta.reshape(heads, count, BLOCK)
    running = jnp.cumsum(decay.reshape(heads, count, BLOCK), axis=-1)
    causal = jnp.tril(jnp.ones((BLOCK, BLOCK), bool))
    strict = jnp.tril(jnp.ones((BLOCK, BLOCK), bool), -1)
    within = jnp.exp(jnp.where(causal, running[..., :, None] - running[..., None, :], -jnp.inf))
    key_beta = key * beta[..., None]
    lower = jnp.where(
        strict,
        jnp.einsum("hnid,hnjd->hnij", key_beta, key, precision=highest_precision) * within,
        0.0,
    )
    system = jnp.eye(BLOCK, dtype=jnp.float32) + lower
    weighted = jax.scipy.linalg.solve_triangular(
        system, key_beta * jnp.exp(running)[..., None], lower=True, unit_diagonal=True
    )
    scores = jnp.einsum("hnid,hnjd->hnij", query, key, precision=highest_precision) * within
    query_decayed = query * jnp.exp(running)[..., None]
    key_decayed = key * jnp.exp(running[..., -1:] - running)[..., None]
    block_decay = jnp.exp(running[..., -1])
    return (system, beta, weighted, query_decayed, key_decayed, scores, block_decay)


def run_blocks(terms, value, start):
    system, beta, weighted, query_decayed, key_decayed, scores, block_decay = terms
    heads, count = (beta.shape[0], beta.shape[1])
    fresh = jax.scipy.linalg.solve_triangular(
        system,
        value.reshape(heads, count, BLOCK, -1) * beta[..., None],
        lower=True,
        unit_diagonal=True,
    )
    missing = start.shape[-1] - fresh.shape[-1]
    fresh = jnp.concatenate([fresh, jnp.zeros(fresh.shape[:-1] + (missing,), jnp.float32)], -1)

    def advance(recurrent_state, inputs):
        (
            fresh_value_block,
            block_weighted_values,
            block_queries,
            block_keys,
            block_scores,
            block_decay_factor,
        ) = inputs
        corrected_value = fresh_value_block - jnp.einsum(
            "nya,nag->nyg", block_weighted_values, recurrent_state, precision=highest_precision
        )
        state_next = block_decay_factor[:, None, None] * recurrent_state + jnp.einsum(
            "iyp,iyu->ipu", block_keys, corrected_value, precision=highest_precision
        )
        final_output = jnp.einsum(
            "nya,nag->nyg", block_queries, recurrent_state, precision=highest_precision
        ) + jnp.einsum("emp,epk->emk", block_scores, corrected_value, precision=highest_precision)
        return (state_next, final_output)

    inputs = tuple(
        (
            jnp.moveaxis(item, 1, 0)
            for item in (fresh, weighted, query_decayed, key_decayed, scores, block_decay)
        )
    )
    final, output_list = lax.scan(advance, start, inputs)
    return (jnp.moveaxis(output_list, 0, 1).reshape(heads, count * BLOCK, -1), final)


def compose(earlier, later):
    return (
        jnp.einsum("hij,hjk->hik", later[0], earlier[0], precision=highest_precision),
        jnp.einsum("hij,hjk->hik", later[0], earlier[1], precision=highest_precision) + later[1],
    )


def slot_places(routes, groups, capacity, experts):
    rows, picks = routes.shape
    flat = routes.reshape(groups, rows // groups * picks)
    matches = (flat[..., None] == jnp.arange(experts, dtype=jnp.int32)).astype(jnp.int32)
    before = jnp.cumsum(matches, axis=1) - matches
    rank = jnp.sum(before * matches, -1)
    group = jnp.arange(groups, dtype=jnp.int32)[:, None]
    return ((flat * groups + group) * capacity + rank).reshape(rows, picks)


def per_device(
    residual_in,
    queries,
    keys,
    values,
    out_gate,
    beta_logit,
    decay_logit,
    decay_log,
    head_gain,
    out_weight,
    norm_gain,
    final_gain,
    expert_index,
    route_weights,
    expert_gate,
    expert_up,
    expert_down,
):
    length, width = residual_in.shape
    heads = beta_logit.shape[0]

    def split_heads(data):
        return data.astype(jnp.float32).reshape(length, heads, HEAD_FEATURES).transpose(1, 0, 2)

    query = unit_rows(split_heads(queries)) * HEAD_FEATURES ** (-0.5)
    key = unit_rows(split_heads(keys))
    value = split_heads(values)
    beta = jax.nn.sigmoid(beta_logit.astype(jnp.float32))
    decay = -jnp.exp(decay_log)[:, None] * jax.nn.softplus(decay_logit.astype(jnp.float32))
    terms = block_terms(query, key, beta, decay)
    identity_map = jnp.broadcast_to(
        jnp.eye(HEAD_FEATURES, dtype=jnp.float32), (heads, HEAD_FEATURES, HEAD_FEATURES)
    )
    blank = jnp.zeros((heads, HEAD_FEATURES, HEAD_FEATURES), jnp.float32)
    extended = jnp.concatenate([blank, identity_map], -1)
    output_list, final = run_blocks(terms, value, extended)
    prefix = carried_in(
        (final[..., HEAD_FEATURES:], final[..., :HEAD_FEATURES]),
        "sp",
        compose,
        (identity_map, blank),
    )
    entry_value = prefix[1]
    mixed = output_list[..., :HEAD_FEATURES] + jnp.einsum(
        "apj,ajz->apz", output_list[..., HEAD_FEATURES:], entry_value, precision=highest_precision
    )
    normalized = mixed * lax.rsqrt(jnp.mean(mixed * mixed, -1, keepdims=True) + 1e-06) * head_gain
    gated = (
        (normalized * jax.nn.silu(split_heads(out_gate)))
        .transpose(1, 0, 2)
        .reshape(length, heads * HEAD_FEATURES)
        .astype(jnp.bfloat16)
    )
    split_count = lax.axis_size("tp")
    expert_count = lax.axis_size("sp") * expert_gate.shape[0]
    rows = length // split_count
    first = lax.axis_index("tp") * rows
    projected = lax.psum_scatter(
        jnp.dot(gated, out_weight, preferred_element_type=jnp.float32).astype(jnp.bfloat16),
        "tp",
        scatter_dimension=0,
        tiled=True,
    ).astype(jnp.float32)
    residual = lax.dynamic_slice_in_dim(residual_in, first, rows, 0)
    routes = lax.dynamic_slice_in_dim(expert_index, first, rows, 0)
    weights = lax.dynamic_slice_in_dim(route_weights, first, rows, 0)
    groups = 1
    capacity = 2 * TOP * (length // split_count) // expert_count
    hidden_in = layer_norm(
        residual_scale * residual.astype(jnp.float32) + projected, norm_gain
    ).astype(jnp.bfloat16)
    places = slot_places(routes, groups, capacity, expert_count)
    slots = expert_count * groups * capacity
    table = (places[:, :, None] == jnp.arange(slots, dtype=jnp.int32)).astype(jnp.bfloat16)
    send = jnp.einsum(
        "rs,rd->sd", jnp.sum(table, 1), hidden_in, preferred_element_type=jnp.float32
    ).astype(jnp.bfloat16)
    arrived = lax.all_to_all(
        send.reshape(expert_count, groups * capacity, width),
        "sp",
        split_axis=0,
        concat_axis=0,
        tiled=True,
    ).reshape(slots, width)
    gate_matrix, up_matrix, down_matrix = (expert_gate[0], expert_up[0], expert_down[0])
    piece = lax.all_gather(arrived, "tp", axis=0, tiled=True)
    gate = jnp.dot(piece, gate_matrix, preferred_element_type=jnp.float32)
    up = jnp.dot(piece, up_matrix, preferred_element_type=jnp.float32)
    inner = (jax.nn.silu(gate) * up).astype(jnp.bfloat16)
    partial_value = jnp.dot(inner, down_matrix, preferred_element_type=jnp.float32)
    result = lax.psum_scatter(
        partial_value.astype(jnp.bfloat16), "tp", scatter_dimension=0, tiled=True
    )
    back = lax.all_to_all(
        result.reshape(expert_count, groups * capacity, width),
        "sp",
        split_axis=0,
        concat_axis=0,
        tiled=True,
    ).reshape(slots, width)
    gathered = jnp.einsum("rks,sd->rkd", table, back, preferred_element_type=jnp.float32)
    routed = jnp.sum(weights[..., None] * gathered, 1)
    layer_out = layer_norm(
        residual_scale * hidden_in.astype(jnp.float32) + routed, final_gain
    ).astype(jnp.bfloat16)
    layer_out = lax.all_gather(layer_out, "tp", axis=0, tiled=True)
    return layer_out


def mm(a, b):
    return jnp.dot(a.astype(jnp.bfloat16), b.astype(jnp.bfloat16), preferred_element_type=jnp.float32)


def mm_nt(a, b):
    return lax.dot_general(
        a.astype(jnp.bfloat16),
        b.astype(jnp.bfloat16),
        (((1,), (1,)), ((), ())),
        preferred_element_type=jnp.float32,
    )


def mm_tn(a, b):
    return lax.dot_general(
        a.astype(jnp.bfloat16),
        b.astype(jnp.bfloat16),
        (((0,), (0,)), ((), ())),
        preferred_element_type=jnp.float32,
    )


def layer_kernel(
    n_sp,
    n_tp,
    residual_ref,
    query_ref,
    key_ref,
    value_ref,
    out_gate_ref,
    beta_ref,
    decay_ref,
    decay_log_ref,
    head_gain_ref,
    norm_gain_ref,
    final_gain_ref,
    index_ref,
    weights_ref,
    out_weight_hbm,
    gate_hbm,
    up_hbm,
    down_hbm,
    out_ref,
    out_weight_v,
    gate_v,
    up_v,
    down_v,
    maps_v,
    adds_v,
    state_in,
    state_out,
    mixed_v,
    readout_v,
    gated_v,
    proj_v,
    proj_in,
    hidden_v,
    send_v,
    arrived_v,
    inner_v,
    part_v,
    part_in,
    pair_v,
    result_v,
    back_v,
    local_sem,
    state_sem,
    proj_sem,
    send_sem,
    fan_sem,
    part_sem,
    back_sem,
    out_sem,
):
    s = lax.axis_index("sp")
    t = lax.axis_index("tp")
    length, width = residual_ref.shape
    heads = beta_ref.shape[0]
    rows = length // n_tp
    chunks, _, group, cap, _ = arrived_v.shape
    half = width // 2
    right, left = slice(half, width), slice(0, half)
    slots = n_sp * cap
    feat = HEAD_FEATURES
    hidden_units = gate_v.shape[1]

    local = [
        pltpu.make_async_copy(out_weight_hbm, out_weight_v, local_sem.at[0]),
        pltpu.make_async_copy(gate_hbm.at[0], gate_v, local_sem.at[1]),
        pltpu.make_async_copy(up_hbm.at[0], up_v, local_sem.at[2]),
        pltpu.make_async_copy(down_hbm.at[0], down_v, local_sem.at[3]),
    ]
    for copy in local:
        copy.start()

    barrier = pltpu.get_barrier_semaphore()
    for k in range(1, n_sp):
        pl.semaphore_signal(
            barrier, inc=1, device_id=(lax.rem(s + k, n_sp), t), device_id_type=MESH
        )
    for k in range(1, n_tp):
        pl.semaphore_signal(
            barrier, inc=1, device_id=(s, lax.rem(t + k, n_tp)), device_id_type=MESH
        )

    def remote(src, dst, sem_a, sem_b, to_s, to_t):
        return pltpu.make_async_remote_copy(
            src_ref=src,
            dst_ref=dst,
            send_sem=sem_a,
            recv_sem=sem_b,
            device_id=(to_s, to_t),
            device_id_type=MESH,
        )

    row_id = lax.broadcasted_iota(jnp.int32, (length, length), 0)
    col_id = lax.broadcasted_iota(jnp.int32, (length, length), 1)
    causal = row_id >= col_id
    strict = row_id > col_id
    eye = (row_id == col_id).astype(jnp.float32)
    tril = causal.astype(jnp.float32)
    beta = jax.nn.sigmoid(beta_ref[...].astype(jnp.float32))
    logit = decay_ref[...].astype(jnp.float32)
    soft = jnp.maximum(logit, 0.0) + jnp.log(1.0 + jnp.exp(-jnp.abs(logit)))
    head_eye = lax.broadcasted_iota(jnp.int32, (heads, heads), 0) == lax.broadcasted_iota(
        jnp.int32, (heads, heads), 1
    )
    rate = jnp.sum(jnp.where(head_eye, jnp.exp(decay_log_ref[...]), 0.0), 1, keepdims=True)
    decay = -rate * soft
    exact = functools.partial(
        lax.dot_general, precision=highest_precision, preferred_element_type=jnp.float32
    )
    nt = (((1,), (1,)), ((), ()))
    run_rows = exact(decay, tril, nt)
    run_cols = exact(tril, decay, nt)
    beta_cols = exact(eye, beta, nt)

    lowers, inverses, rights, score_list, q_list, kd_list, last_list = [], [], [], [], [], [], []
    for h in range(heads):
        cols = slice(h * feat, (h + 1) * feat)
        query = unit_rows(query_ref[:, cols].astype(jnp.float32)) * feat ** (-0.5)
        key = unit_rows(key_ref[:, cols].astype(jnp.float32))
        value = value_ref[:, cols].astype(jnp.float32)
        run_c = run_cols[:, h : h + 1]
        run_r = run_rows[h : h + 1, :]
        beta_c = beta_cols[:, h : h + 1]
        last = run_cols[length - 1 : length, h : h + 1]
        within = jnp.where(causal, jnp.exp(jnp.minimum(run_c - run_r, 0.0)), 0.0)
        lowers.append(jnp.where(strict, mm_nt(key, key) * within * beta_c, 0.0))
        score_list.append((mm_nt(query, key) * within).astype(jnp.bfloat16))
        grown = jnp.exp(run_c)
        rights.append(
            jnp.concatenate([value * beta_c, key * (beta_c * grown)], 1).astype(jnp.bfloat16)
        )
        q_list.append(query * grown)
        kd_list.append((key * jnp.exp(last - run_c)).astype(jnp.bfloat16))
        last_list.append(jnp.exp(last))

    def level(size):
        mid = size // 2
        return (row_id // size == col_id // size) & (row_id % size >= mid) & (col_id % size < mid)

    first = level(2)
    inverses = [eye - jnp.where(first, low, 0.0) for low in lowers]
    size = 4
    while size <= length:
        mask = level(size)
        steps = [mm(jnp.where(mask, low, 0.0), inv) for low, inv in zip(lowers, inverses)]
        inverses = [inv - mm(inv, step) for inv, step in zip(inverses, steps)]
        size *= 2
    solved = [mm(inv, right).astype(jnp.bfloat16) for inv, right in zip(inverses, rights)]
    for h in range(heads):
        ends = mm_tn(kd_list[h], solved[h])
        adds_v[h] = ends[:, :feat]
        maps_v[h] = (last_list[h] * eye[:feat, :feat] - ends[:, feat:]).astype(jnp.bfloat16)
    for h in range(heads):
        seen = mm(score_list[h], solved[h])
        mixed_v[h] = seen[:, :feat]
        readout_v[h] = (q_list[h] - seen[:, feat:]).astype(jnp.bfloat16)

    pl.semaphore_wait(barrier, n_sp - 1 + n_tp - 1)

    after = lax.rem(s + 1, n_sp)

    def state_copy(h):
        return remote(
            state_out.at[h], state_in.at[h], state_sem.at[0, h], state_sem.at[1, h], after, t
        )

    @pl.when(s == 0)
    def _():
        state_in[...] = jnp.zeros_like(state_in)

    for h in range(heads):

        @pl.when(s > 0)
        def _():
            state_copy(h).wait_recv()

        @pl.when(s < n_sp - 1)
        def _():
            state_out[h] = (mm(maps_v[h], state_in[h]) + adds_v[h]).astype(jnp.bfloat16)
            state_copy(h).start()

    for h in range(heads):
        cols = slice(h * feat, (h + 1) * feat)
        mixed = mixed_v[h] + mm(readout_v[h], state_in[h])
        normalized = (
            mixed * lax.rsqrt(jnp.mean(mixed * mixed, -1, keepdims=True) + 1e-06) * head_gain_ref[...]
        )
        gate = out_gate_ref[:, cols].astype(jnp.float32)
        gated_v[:, cols] = (normalized * (gate * jax.nn.sigmoid(gate))).astype(jnp.bfloat16)

    local[0].wait()

    def project(i, carry):
        cols = pl.ds(pl.multiple_of(i * 512, 512), 512)
        proj_v[:, cols] = jnp.dot(
            gated_v[...], out_weight_v[:, cols], preferred_element_type=jnp.float32
        ).astype(jnp.bfloat16)
        return carry

    lax.fori_loop(0, width // 512, project, 0)

    def row_block(i):
        return pl.ds(pl.multiple_of(i * rows, rows), rows)

    proj_copies = []
    for k in range(1, n_tp):
        to = lax.rem(t + k, n_tp)
        copy = remote(
            proj_v.at[row_block(to)], proj_in.at[k - 1], proj_sem.at[0, k - 1], proj_sem.at[1, k - 1], s, to
        )
        copy.start()
        proj_copies.append(copy)

    own_row = (
        lax.broadcasted_iota(jnp.int32, (rows, length), 1)
        == lax.broadcasted_iota(jnp.int32, (rows, length), 0) + t * rows
    ).astype(jnp.float32)
    index = exact(own_row, index_ref[...].astype(jnp.float32), nt)
    weights = exact(own_row, weights_ref[...], nt)
    slot_id = lax.broadcasted_iota(jnp.int32, (rows, slots), 1)
    owner = (slot_id // cap).astype(jnp.float32)
    picks = [(index[:, j : j + 1] == owner).astype(jnp.float32) for j in range(TOP)]
    both = functools.reduce(jnp.add, picks)
    earlier = (
        lax.broadcasted_iota(jnp.int32, (rows, rows), 0)
        > lax.broadcasted_iota(jnp.int32, (rows, rows), 1)
    ).astype(jnp.float32)
    rank = mm(earlier, both)
    here = (rank == (slot_id % cap).astype(jnp.float32)).astype(jnp.float32)
    tables = [(pick * here).astype(jnp.bfloat16) for pick in picks]
    table = (both * here).astype(jnp.bfloat16)

    tx = t + 1 - 2 * lax.rem(t, 2)
    ty = lax.rem(t + 2, 4)
    td = lax.rem(tx + 2, 4)

    def send_copy(to):
        return remote(
            send_v.at[to],
            arrived_v.at[s // group, t, s % group],
            send_sem.at[0, to],
            send_sem.at[1, s],
            to,
            t,
        )

    def arrival(p):
        return remote(
            send_v.at[p],
            arrived_v.at[p // group, t, p % group],
            send_sem.at[0, p],
            send_sem.at[1, p],
            p,
            t,
        )

    def fan_copies(c):
        mine = arrived_v.at[c, t]
        return [
            remote(mine, mine, fan_sem.at[0, 0, c], fan_sem.at[0, 1, c], s, tx),
            remote(mine, mine, fan_sem.at[1, 0, c], fan_sem.at[1, 1, c], s, ty),
        ]

    def relay_copies(c):
        a = arrived_v.at[c, tx, :, :, left]
        b = arrived_v.at[c, ty, :, :, right]
        return [
            remote(a, a, fan_sem.at[2, 0, c], fan_sem.at[2, 1, c], s, ty),
            remote(b, b, fan_sem.at[3, 0, c], fan_sem.at[3, 1, c], s, tx),
        ]

    def fan_out(c):
        for p in range(c * group, (c + 1) * group):

            @pl.when(s != p)
            def _():
                arrival(p).wait_recv()

        for copy in fan_copies(c):
            copy.start()

    def relay(c):
        for copy, onward in zip(fan_copies(c), relay_copies(c)):
            copy.wait_recv()
            onward.start()

    home = s // group

    @pl.when(home >= 2)
    def _():
        fan_out(0)

    projected = proj_v[row_block(t), :].astype(jnp.float32)
    for k in range(1, n_tp):
        proj_copies[k - 1].wait_recv()
        projected = projected + proj_in[k - 1].astype(jnp.float32)
    residual = residual_ref[row_block(t), :].astype(jnp.float32)
    hidden_in = layer_norm(residual_scale * residual + projected, norm_gain_ref[...]).astype(
        jnp.bfloat16
    )
    hidden_v[...] = hidden_in

    send_v[...] = mm_tn(table, hidden_in).astype(jnp.bfloat16).reshape(n_sp, cap, width)

    for k in range(1, n_sp):
        send_copy(lax.rem(s + k, n_sp)).start()
    arrived_v[home, t, s % group] = send_v[s]

    def part_copies(c):
        def one(kind, src, to):
            return remote(
                src, part_in.at[kind, c], part_sem.at[kind, 0, c], part_sem.at[kind, 1, c], s, to
            )

        return [
            one(0, part_v.at[c, td, :, left], tx),
            one(1, part_v.at[c, td, :, right], ty),
            one(2, part_v.at[c, tx, :, left], tx),
            one(3, part_v.at[c, ty, :, right], ty),
            one(4, pair_v.at[0, c], ty),
            one(5, pair_v.at[1, c], tx),
        ]

    def gate_up(c):
        piece = arrived_v[c].reshape(n_tp * group * cap, width)

        def step(i, carry):
            cols = pl.ds(pl.multiple_of(i * 256, 256), 256)
            gate = jnp.dot(piece, gate_v[:, cols], preferred_element_type=jnp.float32)
            up = jnp.dot(piece, up_v[:, cols], preferred_element_type=jnp.float32)
            inner_v[:, cols] = (gate * jax.nn.sigmoid(gate) * up).astype(jnp.bfloat16)
            return carry

        lax.fori_loop(0, hidden_units // 256, step, 0)

    def down(c):
        def step(i, carry):
            cols = pl.ds(pl.multiple_of(i * 512, 512), 512)
            part_v[c, :, :, cols] = (
                jnp.dot(inner_v[...], down_v[:, cols], preferred_element_type=jnp.float32)
                .astype(jnp.bfloat16)
                .reshape(n_tp, group * cap, 512)
            )
            return carry

        lax.fori_loop(0, width // 512, step, 0)

    def pair_up(c):
        copies = part_copies(c)
        wide = jnp.float32
        copies[0].wait_recv()
        pair_v[0, c] = (part_v[c, ty, :, left].astype(wide) + part_in[0, c].astype(wide)).astype(
            jnp.bfloat16
        )
        copies[4].start()
        copies[1].wait_recv()
        pair_v[1, c] = (part_v[c, tx, :, right].astype(wide) + part_in[1, c].astype(wide)).astype(
            jnp.bfloat16
        )
        copies[5].start()

    def back_copy(c, i):
        return remote(
            result_v.at[c, i],
            back_v.at[s],
            back_sem.at[0, c * group + i],
            back_sem.at[1, s],
            c * group + i,
            t,
        )

    def finish(c):
        copies = part_copies(c)
        for i in range(2, 6):
            copies[i].wait_recv()
        own = part_v[c, t].astype(jnp.float32)
        near, far = part_in[2, c].astype(jnp.float32), part_in[4, c].astype(jnp.float32)
        low = own[:, left] + near + far
        near, far = part_in[3, c].astype(jnp.float32), part_in[5, c].astype(jnp.float32)
        high = own[:, right] + near + far
        result_v[c, :, :, left] = low.astype(jnp.bfloat16).reshape(group, cap, half)
        result_v[c, :, :, right] = high.astype(jnp.bfloat16).reshape(group, cap, half)
        for i in range(group):
            p = c * group + i

            @pl.when(s != p)
            def _():
                back_copy(c, i).start()

            @pl.when(s == p)
            def _():
                back_v[p] = result_v[c, i]

    @pl.when(home < 2)
    def _():
        fan_out(0)

    relay(0)
    if chunks > 1:
        fan_out(1)
    for copy in local[1:]:
        copy.wait()
    for i in range(chunks + 2):
        if i < chunks:
            for copy in relay_copies(i):
                copy.wait_recv()
            gate_up(i)
            if i + 1 < chunks:
                relay(i + 1)
            if i + 2 < chunks:
                fan_out(i + 2)
            down(i)
            for copy in part_copies(i)[:4]:
                copy.start()
        if 1 <= i <= chunks:
            pair_up(i - 1)
        if i >= 2:
            finish(i - 2)

    for p in range(n_sp):

        @pl.when(s != p)
        def _():
            remote(
                result_v.at[0, 0], back_v.at[p], back_sem.at[0, p], back_sem.at[1, p], p, t
            ).wait_recv()

    back = back_v[...].reshape(slots, width)
    routed = jnp.zeros((rows, width), jnp.float32)
    for j in range(TOP):
        routed = routed + weights[:, j : j + 1] * mm(tables[j], back)
    out_ref[row_block(t), :] = layer_norm(
        residual_scale * hidden_v[...].astype(jnp.float32) + routed, final_gain_ref[...]
    ).astype(jnp.bfloat16)

    out_copies = []
    for k in range(1, n_tp):
        copy = remote(
            out_ref.at[row_block(t)],
            out_ref.at[row_block(t)],
            out_sem.at[0, k - 1],
            out_sem.at[1, k - 1],
            s,
            lax.rem(t + k, n_tp),
        )
        copy.start()
        out_copies.append(copy)

    @pl.when(s < n_sp - 1)
    def _():
        for h in range(heads):
            state_copy(h).wait_send()

    for copy in proj_copies:
        copy.wait_send()
    for k in range(1, n_sp):
        send_copy(lax.rem(s + k, n_sp)).wait_send()
    for c in range(chunks):
        for copy in fan_copies(c) + relay_copies(c) + part_copies(c):
            copy.wait_send()
        for i in range(group):

            @pl.when(s != c * group + i)
            def _():
                back_copy(c, i).wait_send()

    for copy in out_copies:
        copy.wait()


def fused(args, n_sp, n_tp, cap):
    (residual_in, queries, keys, values, out_gate, beta_logit, decay_logit, decay_log, head_gain,
     out_weight, norm_gain, final_gain, expert_index, route_weights, expert_gate, expert_up,
     expert_down) = args
    length, width = residual_in.shape
    heads = beta_logit.shape[0]
    rows = length // n_tp
    chunks = n_sp // GROUP
    units = expert_gate.shape[2]
    feat = HEAD_FEATURES
    low, full = jnp.bfloat16, jnp.float32
    vmem = pl.BlockSpec(memory_space=pltpu.VMEM)
    hbm = pl.BlockSpec(memory_space=pl.ANY)
    dma = pltpu.SemaphoreType.DMA
    return pl.pallas_call(
        functools.partial(layer_kernel, n_sp, n_tp),
        out_shape=pltpu.VMEM((length, width), low),
        in_specs=[vmem] * 13 + [hbm] * 4,
        out_specs=vmem,
        scratch_shapes=[
            pltpu.VMEM(out_weight.shape, low),
            pltpu.VMEM(expert_gate.shape[1:], low),
            pltpu.VMEM(expert_up.shape[1:], low),
            pltpu.VMEM(expert_down.shape[1:], low),
            pltpu.VMEM((heads, feat, feat), low),
            pltpu.VMEM((heads, feat, feat), full),
            pltpu.VMEM((heads, feat, feat), low),
            pltpu.VMEM((heads, feat, feat), low),
            pltpu.VMEM((heads, length, feat), full),
            pltpu.VMEM((heads, length, feat), low),
            pltpu.VMEM((length, heads * feat), low),
            pltpu.VMEM((length, width), low),
            pltpu.VMEM((n_tp - 1, rows, width), low),
            pltpu.VMEM((rows, width), low),
            pltpu.VMEM((n_sp, cap, width), low),
            pltpu.VMEM((chunks, n_tp, GROUP, cap, width), low),
            pltpu.VMEM((n_tp * GROUP * cap, units), low),
            pltpu.VMEM((chunks, n_tp, GROUP * cap, width), low),
            pltpu.VMEM((6, chunks, GROUP * cap, width // 2), low),
            pltpu.VMEM((2, chunks, GROUP * cap, width // 2), low),
            pltpu.VMEM((chunks, GROUP, cap, width), low),
            pltpu.VMEM((n_sp, cap, width), low),
            dma((4,)),
            dma((2, heads)),
            dma((2, n_tp - 1)),
            dma((2, n_sp)),
            dma((4, 2, chunks)),
            dma((6, 2, chunks)),
            dma((2, n_sp)),
            dma((2, n_tp - 1)),
        ],
        compiler_params=pltpu.CompilerParams(
            collective_id=0, has_side_effects=True, vmem_limit_bytes=60 * 1024 * 1024
        ),
    )(
        residual_in, queries, keys, values, out_gate, beta_logit, decay_logit,
        decay_log.reshape(1, heads), head_gain.reshape(1, -1), norm_gain.reshape(1, -1),
        final_gain.reshape(1, -1), expert_index.T, route_weights.T, out_weight, expert_gate,
        expert_up, expert_down,
    )


def any_size(*args):
    n_sp, n_tp = lax.axis_size("sp"), lax.axis_size("tp")
    residual_in, expert_gate = args[0], args[14]
    length, width = residual_in.shape
    experts = n_sp * expert_gate.shape[0]
    cap = 2 * TOP * (length // n_tp) // experts
    fits = (
        expert_gate.shape[0] == 1
        and n_sp > GROUP
        and n_sp % GROUP == 0
        and n_tp == 4
        and length == HEAD_FEATURES
        and cap % 16 == 0
        and (length // n_tp) % 16 == 0
        and (n_sp * cap) % 128 == 0
        and width % 512 == 0
        and expert_gate.shape[2] % 256 == 0
    )
    return fused(args, n_sp, n_tp, cap) if fits else per_device(*args)


def solution(mesh):
    in_specs = (
        P("sp", None),
        P("sp", "tp"),
        P("sp", "tp"),
        P("sp", "tp"),
        P("sp", "tp"),
        P("tp", "sp"),
        P("tp", "sp"),
        P("tp"),
        P(),
        P("tp", None),
        P(),
        P(),
        P("sp", None),
        P("sp", None),
        P("sp", None, "tp"),
        P("sp", None, "tp"),
        P("sp", "tp", None),
    )
    out_specs = P("sp", None)
    return jax.shard_map(
        any_size, mesh=mesh, in_specs=in_specs, out_specs=out_specs, check_vma=False
    )
```

```python
import functools

import jax
import jax.numpy as jnp
from jax import lax
from jax.experimental import pallas as pl
from jax.experimental.pallas import tpu as pltpu
from jax.sharding import PartitionSpec as P

MESH = pl.DeviceIdType.MESH

HEAD_FEATURES = 128
TOP = 2
BLOCK = 64
GROUP = 2
VISITS = ((1, 0, 3, 2), (0, 2, 3, 1), (0, 1, 3, 2), (2, 1, 0, 3))
FAR = ((1, 3, 2), (0, 2, 3), (0, 1, 3), (2, 1, 0))


highest_precision = lax.Precision.HIGHEST
residual_scale = 2.0**0.5


def carried_in(x, axis, join, neutral):
    place = lax.axis_index(axis)
    gathered = jax.tree.map(
        lambda a, kind: lax.all_gather(a.astype(kind), axis), x, (jnp.bfloat16, jnp.bfloat16)
    )
    state = jax.tree.map(lambda a, e: jnp.zeros_like(a) + jnp.asarray(e, a.dtype), x, neutral)

    def one(turn, state):
        return join(
            state,
            jax.tree.map(
                lambda a, own: lax.dynamic_index_in_dim(a, turn, 0, False).astype(own.dtype),
                gathered,
                x,
            ),
        )

    return lax.fori_loop(0, place, one, state)


def unit_rows(data):
    return data * lax.rsqrt(jnp.sum(data * data, -1, keepdims=True) + 1e-06)


def layer_norm(data, gain):
    center = data - jnp.mean(data, -1, keepdims=True)
    return center * lax.rsqrt(jnp.mean(center * center, -1, keepdims=True) + 1e-05) * gain


def block_terms(query, key, beta, decay):
    heads, length, width = query.shape
    count = length // BLOCK
    shape = (heads, count, BLOCK, width)
    query = query.reshape(shape)
    key = key.reshape(shape)
    beta = beta.reshape(heads, count, BLOCK)
    running = jnp.cumsum(decay.reshape(heads, count, BLOCK), axis=-1)
    causal = jnp.tril(jnp.ones((BLOCK, BLOCK), bool))
    strict = jnp.tril(jnp.ones((BLOCK, BLOCK), bool), -1)
    within = jnp.exp(jnp.where(causal, running[..., :, None] - running[..., None, :], -jnp.inf))
    key_beta = key * beta[..., None]
    lower = jnp.where(
        strict,
        jnp.einsum("hnid,hnjd->hnij", key_beta, key, precision=highest_precision) * within,
        0.0,
    )
    system = jnp.eye(BLOCK, dtype=jnp.float32) + lower
    weighted = jax.scipy.linalg.solve_triangular(
        system, key_beta * jnp.exp(running)[..., None], lower=True, unit_diagonal=True
    )
    scores = jnp.einsum("hnid,hnjd->hnij", query, key, precision=highest_precision) * within
    query_decayed = query * jnp.exp(running)[..., None]
    key_decayed = key * jnp.exp(running[..., -1:] - running)[..., None]
    block_decay = jnp.exp(running[..., -1])
    return (system, beta, weighted, query_decayed, key_decayed, scores, block_decay)


def run_blocks(terms, value, start):
    system, beta, weighted, query_decayed, key_decayed, scores, block_decay = terms
    heads, count = (beta.shape[0], beta.shape[1])
    fresh = jax.scipy.linalg.solve_triangular(
        system,
        value.reshape(heads, count, BLOCK, -1) * beta[..., None],
        lower=True,
        unit_diagonal=True,
    )
    missing = start.shape[-1] - fresh.shape[-1]
    fresh = jnp.concatenate([fresh, jnp.zeros(fresh.shape[:-1] + (missing,), jnp.float32)], -1)

    def advance(recurrent_state, inputs):
        (
            fresh_value_block,
            block_weighted_values,
            block_queries,
            block_keys,
            block_scores,
            block_decay_factor,
        ) = inputs
        corrected_value = fresh_value_block - jnp.einsum(
            "nya,nag->nyg", block_weighted_values, recurrent_state, precision=highest_precision
        )
        state_next = block_decay_factor[:, None, None] * recurrent_state + jnp.einsum(
            "iyp,iyu->ipu", block_keys, corrected_value, precision=highest_precision
        )
        final_output = jnp.einsum(
            "nya,nag->nyg", block_queries, recurrent_state, precision=highest_precision
        ) + jnp.einsum("emp,epk->emk", block_scores, corrected_value, precision=highest_precision)
        return (state_next, final_output)

    inputs = tuple(
        (
            jnp.moveaxis(item, 1, 0)
            for item in (fresh, weighted, query_decayed, key_decayed, scores, block_decay)
        )
    )
    final, output_list = lax.scan(advance, start, inputs)
    return (jnp.moveaxis(output_list, 0, 1).reshape(heads, count * BLOCK, -1), final)


def compose(earlier, later):
    return (
        jnp.einsum("hij,hjk->hik", later[0], earlier[0], precision=highest_precision),
        jnp.einsum("hij,hjk->hik", later[0], earlier[1], precision=highest_precision) + later[1],
    )


def slot_places(routes, groups, capacity, experts):
    rows, picks = routes.shape
    flat = routes.reshape(groups, rows // groups * picks)
    matches = (flat[..., None] == jnp.arange(experts, dtype=jnp.int32)).astype(jnp.int32)
    before = jnp.cumsum(matches, axis=1) - matches
    rank = jnp.sum(before * matches, -1)
    group = jnp.arange(groups, dtype=jnp.int32)[:, None]
    return ((flat * groups + group) * capacity + rank).reshape(rows, picks)


def per_device(
    residual_in,
    queries,
    keys,
    values,
    out_gate,
    beta_logit,
    decay_logit,
    decay_log,
    head_gain,
    out_weight,
    norm_gain,
    final_gain,
    expert_index,
    route_weights,
    expert_gate,
    expert_up,
    expert_down,
):
    length, width = residual_in.shape
    heads = beta_logit.shape[0]

    def split_heads(data):
        return data.astype(jnp.float32).reshape(length, heads, HEAD_FEATURES).transpose(1, 0, 2)

    query = unit_rows(split_heads(queries)) * HEAD_FEATURES ** (-0.5)
    key = unit_rows(split_heads(keys))
    value = split_heads(values)
    beta = jax.nn.sigmoid(beta_logit.astype(jnp.float32))
    decay = -jnp.exp(decay_log)[:, None] * jax.nn.softplus(decay_logit.astype(jnp.float32))
    terms = block_terms(query, key, beta, decay)
    identity_map = jnp.broadcast_to(
        jnp.eye(HEAD_FEATURES, dtype=jnp.float32), (heads, HEAD_FEATURES, HEAD_FEATURES)
    )
    blank = jnp.zeros((heads, HEAD_FEATURES, HEAD_FEATURES), jnp.float32)
    extended = jnp.concatenate([blank, identity_map], -1)
    output_list, final = run_blocks(terms, value, extended)
    prefix = carried_in(
        (final[..., HEAD_FEATURES:], final[..., :HEAD_FEATURES]),
        "sp",
        compose,
        (identity_map, blank),
    )
    entry_value = prefix[1]
    mixed = output_list[..., :HEAD_FEATURES] + jnp.einsum(
        "apj,ajz->apz", output_list[..., HEAD_FEATURES:], entry_value, precision=highest_precision
    )
    normalized = mixed * lax.rsqrt(jnp.mean(mixed * mixed, -1, keepdims=True) + 1e-06) * head_gain
    gated = (
        (normalized * jax.nn.silu(split_heads(out_gate)))
        .transpose(1, 0, 2)
        .reshape(length, heads * HEAD_FEATURES)
        .astype(jnp.bfloat16)
    )
    split_count = lax.axis_size("tp")
    expert_count = lax.axis_size("sp") * expert_gate.shape[0]
    rows = length // split_count
    first = lax.axis_index("tp") * rows
    projected = lax.psum_scatter(
        jnp.dot(gated, out_weight, preferred_element_type=jnp.float32).astype(jnp.bfloat16),
        "tp",
        scatter_dimension=0,
        tiled=True,
    ).astype(jnp.float32)
    residual = lax.dynamic_slice_in_dim(residual_in, first, rows, 0)
    routes = lax.dynamic_slice_in_dim(expert_index, first, rows, 0)
    weights = lax.dynamic_slice_in_dim(route_weights, first, rows, 0)
    groups = 1
    capacity = 2 * TOP * (length // split_count) // expert_count
    hidden_in = layer_norm(
        residual_scale * residual.astype(jnp.float32) + projected, norm_gain
    ).astype(jnp.bfloat16)
    places = slot_places(routes, groups, capacity, expert_count)
    slots = expert_count * groups * capacity
    table = (places[:, :, None] == jnp.arange(slots, dtype=jnp.int32)).astype(jnp.bfloat16)
    send = jnp.einsum(
        "rs,rd->sd", jnp.sum(table, 1), hidden_in, preferred_element_type=jnp.float32
    ).astype(jnp.bfloat16)
    arrived = lax.all_to_all(
        send.reshape(expert_count, groups * capacity, width),
        "sp",
        split_axis=0,
        concat_axis=0,
        tiled=True,
    ).reshape(slots, width)
    gate_matrix, up_matrix, down_matrix = (expert_gate[0], expert_up[0], expert_down[0])
    piece = lax.all_gather(arrived, "tp", axis=0, tiled=True)
    gate = jnp.dot(piece, gate_matrix, preferred_element_type=jnp.float32)
    up = jnp.dot(piece, up_matrix, preferred_element_type=jnp.float32)
    inner = (jax.nn.silu(gate) * up).astype(jnp.bfloat16)
    partial_value = jnp.dot(inner, down_matrix, preferred_element_type=jnp.float32)
    result = lax.psum_scatter(
        partial_value.astype(jnp.bfloat16), "tp", scatter_dimension=0, tiled=True
    )
    back = lax.all_to_all(
        result.reshape(expert_count, groups * capacity, width),
        "sp",
        split_axis=0,
        concat_axis=0,
        tiled=True,
    ).reshape(slots, width)
    gathered = jnp.einsum("rks,sd->rkd", table, back, preferred_element_type=jnp.float32)
    routed = jnp.sum(weights[..., None] * gathered, 1)
    layer_out = layer_norm(
        residual_scale * hidden_in.astype(jnp.float32) + routed, final_gain
    ).astype(jnp.bfloat16)
    layer_out = lax.all_gather(layer_out, "tp", axis=0, tiled=True)
    return layer_out


def mm(a, b):
    return jnp.dot(a.astype(jnp.bfloat16), b.astype(jnp.bfloat16), preferred_element_type=jnp.float32)


def mm_nt(a, b):
    return lax.dot_general(
        a.astype(jnp.bfloat16),
        b.astype(jnp.bfloat16),
        (((1,), (1,)), ((), ())),
        preferred_element_type=jnp.float32,
    )


def mm_tn(a, b):
    return lax.dot_general(
        a.astype(jnp.bfloat16),
        b.astype(jnp.bfloat16),
        (((0,), (0,)), ((), ())),
        preferred_element_type=jnp.float32,
    )


scope = jax.named_scope


def pick(table, home):
    chosen = []
    for i in range(len(table[0])):
        value = 0
        for h, order in enumerate(table):
            value = value + (home == h).astype(jnp.int32) * order[i]
        chosen.append(value)
    return chosen


def drain(ref, sem):
    pltpu.make_async_copy(ref, ref, sem).wait()


def layer_kernel(
    n_sp,
    n_tp,
    residual_ref,
    query_ref,
    key_ref,
    value_ref,
    out_gate_ref,
    beta_ref,
    decay_ref,
    decay_log_ref,
    head_gain_ref,
    norm_gain_ref,
    final_gain_ref,
    index_ref,
    weights_ref,
    out_weight_hbm,
    gate_hbm,
    up_hbm,
    down_hbm,
    out_ref,
    out_weight_v,
    gate_v,
    up_v,
    down_v,
    maps_v,
    adds_v,
    state_in,
    state_out,
    mate_out,
    mate_in,
    entry_v,
    mixed_v,
    readout_v,
    gated_v,
    proj_v,
    proj_in,
    hidden_v,
    send_v,
    arrived_v,
    inner_v,
    part_v,
    part_in,
    pair_v,
    result_v,
    back_v,
    final_v,
    local_sem,
    sent_sem,
    state_sem,
    mate_sem,
    entry_sem,
    proj_sem,
    arrive_sem,
    near_sem,
    full_sem,
    pair_sem,
    part_sem,
    back_sem,
    out_sem,
):
    s = lax.axis_index("sp")
    t = lax.axis_index("tp")
    length, width = residual_ref.shape
    heads = beta_ref.shape[0]
    rows = length // n_tp
    chunks, _, group, cap, _ = arrived_v.shape
    half = width // 2
    right, left = slice(half, width), slice(0, half)
    slots = n_sp * cap
    feat = HEAD_FEATURES
    hidden_units = gate_v.shape[1]

    with scope("a_start"):
        pass
    local = [
        pltpu.make_async_copy(out_weight_hbm, out_weight_v, local_sem.at[0]),
        pltpu.make_async_copy(gate_hbm.at[0], gate_v, local_sem.at[1]),
        pltpu.make_async_copy(up_hbm.at[0], up_v, local_sem.at[2]),
        pltpu.make_async_copy(down_hbm.at[0], down_v, local_sem.at[3]),
    ]
    for copy in local:
        copy.start()

    barrier = pltpu.get_barrier_semaphore()
    for k in range(1, n_sp):
        pl.semaphore_signal(
            barrier, inc=1, device_id=(lax.rem(s + k, n_sp), t), device_id_type=MESH
        )
    for k in range(1, n_tp):
        pl.semaphore_signal(
            barrier, inc=1, device_id=(s, lax.rem(t + k, n_tp)), device_id_type=MESH
        )

    def remote(src, dst, sem_a, sem_b, to_s, to_t):
        return pltpu.make_async_remote_copy(
            src_ref=src,
            dst_ref=dst,
            send_sem=sem_a,
            recv_sem=sem_b,
            device_id=(to_s, to_t),
            device_id_type=MESH,
        )

    row_id = lax.broadcasted_iota(jnp.int32, (length, length), 0)
    col_id = lax.broadcasted_iota(jnp.int32, (length, length), 1)
    causal = row_id >= col_id
    strict = row_id > col_id
    eye = (row_id == col_id).astype(jnp.float32)
    tril = causal.astype(jnp.float32)
    beta = jax.nn.sigmoid(beta_ref[...].astype(jnp.float32))
    logit = decay_ref[...].astype(jnp.float32)
    soft = jnp.maximum(logit, 0.0) + jnp.log(1.0 + jnp.exp(-jnp.abs(logit)))
    head_eye = lax.broadcasted_iota(jnp.int32, (heads, heads), 0) == lax.broadcasted_iota(
        jnp.int32, (heads, heads), 1
    )
    rate = jnp.sum(jnp.where(head_eye, jnp.exp(decay_log_ref[...]), 0.0), 1, keepdims=True)
    decay = -rate * soft
    exact = functools.partial(
        lax.dot_general, precision=highest_precision, preferred_element_type=jnp.float32
    )
    nt = (((1,), (1,)), ((), ()))
    run_rows = exact(decay, tril, nt)
    run_cols = exact(tril, decay, nt)
    beta_cols = exact(eye, beta, nt)

    lowers, inverses, rights, score_list, q_list, kd_list, last_list = [], [], [], [], [], [], []
    for h in range(heads):
        cols = slice(h * feat, (h + 1) * feat)
        query = unit_rows(query_ref[:, cols].astype(jnp.float32)) * feat ** (-0.5)
        key = unit_rows(key_ref[:, cols].astype(jnp.float32))
        value = value_ref[:, cols].astype(jnp.float32)
        run_c = run_cols[:, h : h + 1]
        run_r = run_rows[h : h + 1, :]
        beta_c = beta_cols[:, h : h + 1]
        last = run_cols[length - 1 : length, h : h + 1]
        within = jnp.where(causal, jnp.exp(jnp.minimum(run_c - run_r, 0.0)), 0.0)
        lowers.append(jnp.where(strict, mm_nt(key, key) * within * beta_c, 0.0))
        score_list.append((mm_nt(query, key) * within).astype(jnp.bfloat16))
        grown = jnp.exp(run_c)
        rights.append(
            jnp.concatenate([value * beta_c, key * (beta_c * grown)], 1).astype(jnp.bfloat16)
        )
        q_list.append(query * grown)
        kd_list.append((key * jnp.exp(last - run_c)).astype(jnp.bfloat16))
        last_list.append(jnp.exp(last))

    def level(size):
        mid = size // 2
        return (row_id // size == col_id // size) & (row_id % size >= mid) & (col_id % size < mid)

    first = level(2)
    inverses = [eye - jnp.where(first, low, 0.0) for low in lowers]
    size = 4
    while size <= length:
        mask = level(size)
        steps = [mm(jnp.where(mask, low, 0.0), inv) for low, inv in zip(lowers, inverses)]
        inverses = [inv - mm(inv, step) for inv, step in zip(inverses, steps)]
        size *= 2
    solved = [mm(inv, right).astype(jnp.bfloat16) for inv, right in zip(inverses, rights)]
    home, core = s // group, s % group
    mate = home * group + (1 - core)
    after = lax.rem(s + group, n_sp)

    def mate_copy(h):
        return remote(
            mate_out.at[h], mate_in.at[h], sent_sem.at[0], mate_sem.at[h], mate, t
        )

    def state_copy(h):
        return remote(
            state_out.at[h], state_in.at[h], sent_sem.at[1], state_sem.at[h], after, t
        )

    def entry_copy(h):
        return remote(
            state_in.at[h], entry_v.at[h], sent_sem.at[2], entry_sem.at[h], mate, t
        )

    for h in range(heads):
        ends = mm_tn(kd_list[h], solved[h])
        adds_v[h] = ends[:, :feat]
        maps = (last_list[h] * eye[:feat, :feat] - ends[:, feat:]).astype(jnp.bfloat16)
        maps_v[h] = maps
        mate_out[h, 0] = maps
        mate_out[h, 1] = ends[:, :feat].astype(jnp.bfloat16)

    with scope("b_barrier"):
        pl.semaphore_wait(barrier, n_sp - 1 + n_tp - 1)

    @pl.when(core == 0)
    def _():
        for h in range(heads):
            mate_copy(h).start()

    for h in range(heads):
        seen = mm(score_list[h], solved[h])
        mixed_v[h] = seen[:, :feat]
        readout_v[h] = (q_list[h] - seen[:, feat:]).astype(jnp.bfloat16)

    @pl.when(core == 1)
    def _():
        for h in range(heads):
            with scope("c_mate"):
                mate_copy(h).wait_recv()

            @pl.when(home == 0)
            def _():
                state_out[h] = (mm(maps_v[h], mate_in[h, 1]) + adds_v[h]).astype(jnp.bfloat16)
                state_copy(h).start()
                entry_v[h] = mate_in[h, 1]

            @pl.when(home > 0)
            def _():
                both = mm(maps_v[h], jnp.concatenate([mate_in[h, 0], mate_in[h, 1]], 1))
                maps_v[h] = both[:, :feat].astype(jnp.bfloat16)
                adds_v[h] = adds_v[h] + both[:, feat:]

        @pl.when(home > 0)
        def _():
            for h in range(heads):
                with scope("c_state"):
                    state_copy(h).wait_recv()

                @pl.when(home < chunks - 1)
                def _():
                    state_out[h] = (mm(maps_v[h], state_in[h]) + adds_v[h]).astype(jnp.bfloat16)
                    state_copy(h).start()

                entry_copy(h).start()

            for h in range(heads):
                entry_v[h] = (
                    mm(mate_in[h, 0], state_in[h]) + mate_in[h, 1].astype(jnp.float32)
                ).astype(jnp.bfloat16)

    @pl.when((core == 0) & (home == 0))
    def _():
        entry_v[...] = jnp.zeros_like(entry_v)

    @pl.when((core == 0) & (home > 0))
    def _():
        for h in range(heads):
            with scope("c_state"):
                entry_copy(h).wait_recv()

    for h in range(heads):
        cols = slice(h * feat, (h + 1) * feat)
        mixed = mixed_v[h] + mm(readout_v[h], entry_v[h])
        normalized = (
            mixed * lax.rsqrt(jnp.mean(mixed * mixed, -1, keepdims=True) + 1e-06) * head_gain_ref[...]
        )
        gate = out_gate_ref[:, cols].astype(jnp.float32)
        gated_v[:, cols] = (normalized * (gate * jax.nn.sigmoid(gate))).astype(jnp.bfloat16)

    local[0].wait()

    def row_block(i):
        return pl.ds(pl.multiple_of(i * rows, rows), rows)

    def project(i, carry):
        cols = pl.ds(pl.multiple_of(i * 512, 512), 512)
        proj_v[:, cols] = jnp.dot(
            gated_v[...], out_weight_v[:, cols], preferred_element_type=jnp.float32
        ).astype(jnp.bfloat16)
        return carry

    for part, cols in enumerate((left, right)):
        steps = half // 512
        with scope("d_project"):
            lax.fori_loop(part * steps, (part + 1) * steps, project, 0)
        for k in range(1, n_tp):
            to = lax.rem(t + k, n_tp)
            copy = remote(
                proj_v.at[row_block(to), cols],
                proj_in.at[k - 1, :, cols],
                sent_sem.at[3],
                proj_sem.at[0],
                s,
                to,
            )
            copy.start()

    own_row = (
        lax.broadcasted_iota(jnp.int32, (rows, length), 1)
        == lax.broadcasted_iota(jnp.int32, (rows, length), 0) + t * rows
    ).astype(jnp.float32)
    index = exact(own_row, index_ref[...].astype(jnp.float32), nt)
    weights = exact(own_row, weights_ref[...], nt)
    slot_id = lax.broadcasted_iota(jnp.int32, (rows, slots), 1)
    owner = (slot_id // cap).astype(jnp.float32)
    picks = [(index[:, j : j + 1] == owner).astype(jnp.float32) for j in range(TOP)]
    both = functools.reduce(jnp.add, picks)
    earlier = (
        lax.broadcasted_iota(jnp.int32, (rows, rows), 0)
        > lax.broadcasted_iota(jnp.int32, (rows, rows), 1)
    ).astype(jnp.float32)
    rank = mm(earlier, both)
    here = (rank == (slot_id % cap).astype(jnp.float32)).astype(jnp.float32)
    tables = [(pick * here).astype(jnp.bfloat16) for pick in picks]
    table = (both * here).astype(jnp.bfloat16)

    tx = t + 1 - 2 * lax.rem(t, 2)
    ty = lax.rem(t + 2, 4)
    td = lax.rem(tx + 2, 4)

    def send_copy(to):
        return remote(
            send_v.at[to], arrived_v.at[home, t, core], sent_sem.at[4], arrive_sem.at[home], to, t
        )

    order = pick(VISITS, home)
    legs = [(home, core, 1), (home, 1 - core, 1)] + [(c, 0, group) for c in pick(FAR, home)]

    def fan_out(j):
        c, low, count = legs[j]
        if j > 0:
            with scope("g_arrive"):
                drain(arrived_v.at[c, t, pl.ds(low, count)], arrive_sem.at[c])

        def one(cols, sem, to):
            mine = arrived_v.at[c, t, pl.ds(low, count), :, cols]
            remote(mine, mine, sent_sem.at[5], sem, s, to).start()

        one(left, near_sem.at[j, 0], tx)
        one(right, near_sem.at[j, 1], ty)
        one(right, full_sem.at[c], tx)
        one(left, full_sem.at[c], ty)

    def relay(j):
        c, low, count = legs[j]
        for i, (near, cols, to) in enumerate(((tx, left, ty), (ty, right, tx))):
            block = arrived_v.at[c, near, pl.ds(low, count), :, cols]
            with scope("h_fan"):
                drain(block, near_sem.at[j, i])
            remote(block, block, sent_sem.at[5], full_sem.at[c], s, to).start()

    def wait_full(k):
        with scope("j_full"):
            drain(arrived_v.at[order[k], pl.ds(0, 2)], full_sem.at[order[k]])

    projected = proj_v[row_block(t), :].astype(jnp.float32)
    with scope("e_proj"):
        drain(proj_in, proj_sem.at[0])
    for k in range(1, n_tp):
        projected = projected + proj_in[k - 1].astype(jnp.float32)
    residual = residual_ref[row_block(t), :].astype(jnp.float32)
    hidden_in = layer_norm(residual_scale * residual + projected, norm_gain_ref[...]).astype(
        jnp.bfloat16
    )
    hidden_v[...] = hidden_in

    send_v[...] = mm_tn(table, hidden_in).astype(jnp.bfloat16).reshape(n_sp, cap, width)

    for i in range(group):

        @pl.when(s != home * group + i)
        def _():
            send_copy(home * group + i).start()

    for far in range(1, chunks):
        for there in (home - far, home + far):

            @pl.when((there >= 0) & (there < chunks))
            def _():
                for i in range(group):
                    send_copy(there * group + i).start()

    arrived_v[home, t, core] = send_v[s]

    def part_copy(kind, j):
        src, to = (
            (part_v.at[j, td, :, left], tx),
            (part_v.at[j, td, :, right], ty),
            (part_v.at[j, tx, :, left], tx),
            (part_v.at[j, ty, :, right], ty),
            (pair_v.at[0, j], ty),
            (pair_v.at[1, j], tx),
        )[kind]
        sem = pair_sem.at[j, kind] if kind < 2 else part_sem.at[j]
        return remote(src, part_in.at[kind, j], sent_sem.at[6], sem, s, to)

    def gate_up(j, part):
        piece = arrived_v[order[j]].reshape(n_tp * group * cap, width)
        steps = hidden_units // 256 // 2

        def step(i, carry):
            cols = pl.ds(pl.multiple_of(i * 256, 256), 256)
            gate = jnp.dot(piece, gate_v[:, cols], preferred_element_type=jnp.float32)
            up = jnp.dot(piece, up_v[:, cols], preferred_element_type=jnp.float32)
            inner_v[:, cols] = (gate * jax.nn.sigmoid(gate) * up).astype(jnp.bfloat16)
            return carry

        with scope("k_gateup"):
            lax.fori_loop(part * steps, (part + 1) * steps, step, 0)

    def down(j):
        def step(i, carry):
            cols = pl.ds(pl.multiple_of(i * 512, 512), 512)
            part_v[j, :, :, cols] = (
                jnp.dot(
                    inner_v[...], down_v[:, cols], preferred_element_type=jnp.float32
                )
                .astype(jnp.bfloat16)
                .reshape(n_tp, group * cap, 512)
            )
            return carry

        steps = half // 512
        for part in range(2):
            with scope("l_down"):
                lax.fori_loop(part * steps, (part + 1) * steps, step, 0)
            part_copy(part, j).start()
            part_copy(2 + part, j).start()

    def pair_up(j):
        wide = jnp.float32
        for i, (near, cols) in enumerate(((ty, left), (tx, right))):
            with scope("m_pair"):
                drain(part_in.at[i, j], pair_sem.at[j, i])
            pair_v[i, j] = (
                part_v[j, near, :, cols].astype(wide) + part_in[i, j].astype(wide)
            ).astype(jnp.bfloat16)
            part_copy(4 + i, j).start()

    def finish(j):
        with scope("n_finish"):
            drain(part_in.at[pl.ds(2, 4), j], part_sem.at[j])
        for i, cols in enumerate((left, right)):
            near = part_in[2 + i, j].astype(jnp.float32)
            far = part_in[4 + i, j].astype(jnp.float32)
            total = part_v[j, t, :, cols].astype(jnp.float32) + near + far
            result_v[j, :, :, cols] = total.astype(jnp.bfloat16).reshape(group, cap, half)
        for i in range(group):
            p = order[j] * group + i

            @pl.when(s != p)
            def _():
                remote(
                    result_v.at[j, i], back_v.at[s], sent_sem.at[7], back_sem.at[0], p, t
                ).start()

            @pl.when(s == p)
            def _():
                back_v[s] = result_v[j, i]

    fan_out(0)
    fan_out(1)

    @pl.when(home == 0)
    def _():
        relay(0)
        relay(1)

    fan_out(2)

    @pl.when(home > 0)
    def _():
        relay(0)
        relay(1)

    for copy in local[1:4]:
        copy.wait()
    relay(2)

    @pl.when(home > 0)
    def _():
        fan_out(3)

    wait_full(0)
    gate_up(0, 0)

    @pl.when(home > 0)
    def _():
        relay(3)
        fan_out(4)

    gate_up(0, 1)

    @pl.when(home == 0)
    def _():
        fan_out(3)

    down(0)
    wait_full(1)
    gate_up(1, 0)

    @pl.when(home > 0)
    def _():
        relay(4)

    gate_up(1, 1)

    @pl.when(home == 0)
    def _():
        relay(3)
        fan_out(4)

    pair_up(0)
    down(1)
    wait_full(2)
    gate_up(2, 0)

    @pl.when(home == 0)
    def _():
        relay(4)

    gate_up(2, 1)
    pair_up(1)
    finish(0)
    down(2)
    wait_full(3)
    gate_up(3, 0)
    gate_up(3, 1)
    pair_up(2)
    finish(1)
    down(3)
    finish(2)
    pair_up(3)
    finish(3)

    with scope("o_back"):
        drain(back_v.at[pl.ds(0, n_sp - 1)], back_sem.at[0])

    back = back_v[...].reshape(slots, width)
    routed = jnp.zeros((rows, width), jnp.float32)
    for j in range(TOP):
        routed = routed + weights[:, j : j + 1] * mm(tables[j], back)
    final_v[...] = layer_norm(
        residual_scale * hidden_v[...].astype(jnp.float32) + routed, final_gain_ref[...]
    ).astype(jnp.bfloat16)

    def out_copy(owner, q, to, sem):
        cols = pl.ds(q * (width // 4), width // 4)
        cells = out_ref.at[row_block(owner), cols]
        source = final_v.at[:, cols] if owner is t else cells
        return remote(source, cells, sent_sem.at[8], out_sem.at[sem], s, to)

    for q in range(4):
        out_copy(t, q, tx, min(q, 2)).start()
        out_copy(t, 3 - q, ty, min(q, 2) + (3 if q < 2 else 0)).start()
    own_copy = pltpu.make_async_copy(final_v, out_ref.at[row_block(t)], local_sem.at[4])
    own_copy.start()
    piece = final_v.at[:, pl.ds(0, width // 4)]
    with scope("q_out"):
        for q in range(2):
            drain(piece, out_sem.at[q])
            out_copy(tx, q, ty, 2).start()
            drain(piece, out_sem.at[3 + q])
            out_copy(ty, 3 - q, tx, 2).start()

    @pl.when(core == 0)
    def _():
        drain(mate_out, sent_sem.at[0])

    @pl.when((core == 1) & (home < chunks - 1))
    def _():
        drain(state_out, sent_sem.at[1])

    @pl.when((core == 1) & (home > 0))
    def _():
        drain(state_in, sent_sem.at[2])

    drain(proj_in, sent_sem.at[3])
    drain(send_v.at[pl.ds(0, n_sp - 1)], sent_sem.at[4])
    drain(arrived_v.at[:, pl.ds(0, 3)], sent_sem.at[5])
    drain(part_in, sent_sem.at[6])
    drain(back_v.at[pl.ds(0, n_sp - 1)], sent_sem.at[7])
    own_copy.wait()
    with scope("r_out"):
        drain(proj_in.at[pl.ds(0, 2)], out_sem.at[2])
    with scope("s_sends"):
        drain(proj_in, sent_sem.at[8])


def fused(args, n_sp, n_tp, cap):
    (residual_in, queries, keys, values, out_gate, beta_logit, decay_logit, decay_log, head_gain,
     out_weight, norm_gain, final_gain, expert_index, route_weights, expert_gate, expert_up,
     expert_down) = args
    length, width = residual_in.shape
    heads = beta_logit.shape[0]
    rows = length // n_tp
    chunks = n_sp // GROUP
    units = expert_gate.shape[2]
    feat = HEAD_FEATURES
    low, full = jnp.bfloat16, jnp.float32
    vmem = pl.BlockSpec(memory_space=pltpu.VMEM)
    hbm = pl.BlockSpec(memory_space=pl.ANY)
    dma = pltpu.SemaphoreType.DMA
    return pl.pallas_call(
        functools.partial(layer_kernel, n_sp, n_tp),
        out_shape=pltpu.VMEM((length, width), low),
        in_specs=[vmem] * 13 + [hbm] * 4,
        out_specs=hbm,
        scratch_shapes=[
            pltpu.VMEM(out_weight.shape, low),
            pltpu.VMEM(expert_gate.shape[1:], low),
            pltpu.VMEM(expert_up.shape[1:], low),
            pltpu.VMEM(expert_down.shape[1:], low),
            pltpu.VMEM((heads, feat, feat), low),
            pltpu.VMEM((heads, feat, feat), full),
            pltpu.VMEM((heads, feat, feat), low),
            pltpu.VMEM((heads, feat, feat), low),
            pltpu.VMEM((heads, 2, feat, feat), low),
            pltpu.VMEM((heads, 2, feat, feat), low),
            pltpu.VMEM((heads, feat, feat), low),
            pltpu.VMEM((heads, length, feat), full),
            pltpu.VMEM((heads, length, feat), low),
            pltpu.VMEM((length, heads * feat), low),
            pltpu.VMEM((length, width), low),
            pltpu.VMEM((n_tp - 1, rows, width), low),
            pltpu.VMEM((rows, width), low),
            pltpu.VMEM((n_sp, cap, width), low),
            pltpu.VMEM((chunks, n_tp, GROUP, cap, width), low),
            pltpu.VMEM((n_tp * GROUP * cap, units), low),
            pltpu.VMEM((chunks, n_tp, GROUP * cap, width), low),
            pltpu.VMEM((6, chunks, GROUP * cap, width // 2), low),
            pltpu.VMEM((2, chunks, GROUP * cap, width // 2), low),
            pltpu.VMEM((chunks, GROUP, cap, width), low),
            pltpu.VMEM((n_sp, cap, width), low),
            pltpu.VMEM((rows, width), low),
            dma((5,)),
            dma((9,)),
            dma((heads,)),
            dma((heads,)),
            dma((heads,)),
            dma((1,)),
            dma((chunks,)),
            dma((chunks + 1, 2)),
            dma((chunks,)),
            dma((chunks, 2)),
            dma((chunks,)),
            dma((1,)),
            dma((5,)),
        ],
        compiler_params=pltpu.CompilerParams(
            collective_id=0, has_side_effects=True, vmem_limit_bytes=60 * 1024 * 1024
        ),
    )(
        residual_in, queries, keys, values, out_gate, beta_logit, decay_logit,
        decay_log.reshape(1, heads), head_gain.reshape(1, -1), norm_gain.reshape(1, -1),
        final_gain.reshape(1, -1), expert_index.T, route_weights.T, out_weight, expert_gate,
        expert_up, expert_down,
    )


def any_size(*args):
    n_sp, n_tp = lax.axis_size("sp"), lax.axis_size("tp")
    residual_in, expert_gate = args[0], args[14]
    length, width = residual_in.shape
    experts = n_sp * expert_gate.shape[0]
    cap = 2 * TOP * (length // n_tp) // experts
    fits = (
        expert_gate.shape[0] == 1
        and n_sp == GROUP * len(VISITS)
        and n_tp == 4
        and length == HEAD_FEATURES
        and cap % 16 == 0
        and (length // n_tp) % 16 == 0
        and (n_sp * cap) % 128 == 0
        and width % 512 == 0
        and expert_gate.shape[2] % 256 == 0
    )
    return fused(args, n_sp, n_tp, cap) if fits else per_device(*args)


def solution(mesh):
    in_specs = (
        P("sp", None),
        P("sp", "tp"),
        P("sp", "tp"),
        P("sp", "tp"),
        P("sp", "tp"),
        P("tp", "sp"),
        P("tp", "sp"),
        P("tp"),
        P(),
        P("tp", None),
        P(),
        P(),
        P("sp", None),
        P("sp", None),
        P("sp", None, "tp"),
        P("sp", None, "tp"),
        P("sp", "tp", None),
    )
    out_specs = P("sp", None)
    return jax.shard_map(
        any_size, mesh=mesh, in_specs=in_specs, out_specs=out_specs, check_vma=False
    )
```

```python
import functools

import jax
import jax.numpy as jnp
from jax import lax
from jax.experimental import pallas as pl
from jax.experimental.pallas import tpu as pltpu
from jax.sharding import PartitionSpec as P

MESH = pl.DeviceIdType.MESH

HEAD_FEATURES = 128
TOP = 2
BLOCK = 64
GROUP = 2
VISITS = ((1, 2, 3, 0), (0, 2, 3, 1), (0, 3, 1, 2), (0, 1, 2, 3))
SENDS = ((1, 2, 3), (0, 2, 3), (3, 0, 1), (2, 0, 1))


highest_precision = lax.Precision.HIGHEST
residual_scale = 2.0**0.5


def carried_in(x, axis, join, neutral):
    place = lax.axis_index(axis)
    gathered = jax.tree.map(
        lambda a, kind: lax.all_gather(a.astype(kind), axis), x, (jnp.bfloat16, jnp.bfloat16)
    )
    state = jax.tree.map(lambda a, e: jnp.zeros_like(a) + jnp.asarray(e, a.dtype), x, neutral)

    def one(turn, state):
        return join(
            state,
            jax.tree.map(
                lambda a, own: lax.dynamic_index_in_dim(a, turn, 0, False).astype(own.dtype),
                gathered,
                x,
            ),
        )

    return lax.fori_loop(0, place, one, state)


def unit_rows(data):
    return data * lax.rsqrt(jnp.sum(data * data, -1, keepdims=True) + 1e-06)


def layer_norm(data, gain):
    center = data - jnp.mean(data, -1, keepdims=True)
    return center * lax.rsqrt(jnp.mean(center * center, -1, keepdims=True) + 1e-05) * gain


def block_terms(query, key, beta, decay):
    heads, length, width = query.shape
    count = length // BLOCK
    shape = (heads, count, BLOCK, width)
    query = query.reshape(shape)
    key = key.reshape(shape)
    beta = beta.reshape(heads, count, BLOCK)
    running = jnp.cumsum(decay.reshape(heads, count, BLOCK), axis=-1)
    causal = jnp.tril(jnp.ones((BLOCK, BLOCK), bool))
    strict = jnp.tril(jnp.ones((BLOCK, BLOCK), bool), -1)
    within = jnp.exp(jnp.where(causal, running[..., :, None] - running[..., None, :], -jnp.inf))
    key_beta = key * beta[..., None]
    lower = jnp.where(
        strict,
        jnp.einsum("hnid,hnjd->hnij", key_beta, key, precision=highest_precision) * within,
        0.0,
    )
    system = jnp.eye(BLOCK, dtype=jnp.float32) + lower
    weighted = jax.scipy.linalg.solve_triangular(
        system, key_beta * jnp.exp(running)[..., None], lower=True, unit_diagonal=True
    )
    scores = jnp.einsum("hnid,hnjd->hnij", query, key, precision=highest_precision) * within
    query_decayed = query * jnp.exp(running)[..., None]
    key_decayed = key * jnp.exp(running[..., -1:] - running)[..., None]
    block_decay = jnp.exp(running[..., -1])
    return (system, beta, weighted, query_decayed, key_decayed, scores, block_decay)


def run_blocks(terms, value, start):
    system, beta, weighted, query_decayed, key_decayed, scores, block_decay = terms
    heads, count = (beta.shape[0], beta.shape[1])
    fresh = jax.scipy.linalg.solve_triangular(
        system,
        value.reshape(heads, count, BLOCK, -1) * beta[..., None],
        lower=True,
        unit_diagonal=True,
    )
    missing = start.shape[-1] - fresh.shape[-1]
    fresh = jnp.concatenate([fresh, jnp.zeros(fresh.shape[:-1] + (missing,), jnp.float32)], -1)

    def advance(recurrent_state, inputs):
        (
            fresh_value_block,
            block_weighted_values,
            block_queries,
            block_keys,
            block_scores,
            block_decay_factor,
        ) = inputs
        corrected_value = fresh_value_block - jnp.einsum(
            "nya,nag->nyg", block_weighted_values, recurrent_state, precision=highest_precision
        )
        state_next = block_decay_factor[:, None, None] * recurrent_state + jnp.einsum(
            "iyp,iyu->ipu", block_keys, corrected_value, precision=highest_precision
        )
        final_output = jnp.einsum(
            "nya,nag->nyg", block_queries, recurrent_state, precision=highest_precision
        ) + jnp.einsum("emp,epk->emk", block_scores, corrected_value, precision=highest_precision)
        return (state_next, final_output)

    inputs = tuple(
        (
            jnp.moveaxis(item, 1, 0)
            for item in (fresh, weighted, query_decayed, key_decayed, scores, block_decay)
        )
    )
    final, output_list = lax.scan(advance, start, inputs)
    return (jnp.moveaxis(output_list, 0, 1).reshape(heads, count * BLOCK, -1), final)


def compose(earlier, later):
    return (
        jnp.einsum("hij,hjk->hik", later[0], earlier[0], precision=highest_precision),
        jnp.einsum("hij,hjk->hik", later[0], earlier[1], precision=highest_precision) + later[1],
    )


def slot_places(routes, groups, capacity, experts):
    rows, picks = routes.shape
    flat = routes.reshape(groups, rows // groups * picks)
    matches = (flat[..., None] == jnp.arange(experts, dtype=jnp.int32)).astype(jnp.int32)
    before = jnp.cumsum(matches, axis=1) - matches
    rank = jnp.sum(before * matches, -1)
    group = jnp.arange(groups, dtype=jnp.int32)[:, None]
    return ((flat * groups + group) * capacity + rank).reshape(rows, picks)


def per_device(
    residual_in,
    queries,
    keys,
    values,
    out_gate,
    beta_logit,
    decay_logit,
    decay_log,
    head_gain,
    out_weight,
    norm_gain,
    final_gain,
    expert_index,
    route_weights,
    expert_gate,
    expert_up,
    expert_down,
):
    length, width = residual_in.shape
    heads = beta_logit.shape[0]

    def split_heads(data):
        return data.astype(jnp.float32).reshape(length, heads, HEAD_FEATURES).transpose(1, 0, 2)

    query = unit_rows(split_heads(queries)) * HEAD_FEATURES ** (-0.5)
    key = unit_rows(split_heads(keys))
    value = split_heads(values)
    beta = jax.nn.sigmoid(beta_logit.astype(jnp.float32))
    decay = -jnp.exp(decay_log)[:, None] * jax.nn.softplus(decay_logit.astype(jnp.float32))
    terms = block_terms(query, key, beta, decay)
    identity_map = jnp.broadcast_to(
        jnp.eye(HEAD_FEATURES, dtype=jnp.float32), (heads, HEAD_FEATURES, HEAD_FEATURES)
    )
    blank = jnp.zeros((heads, HEAD_FEATURES, HEAD_FEATURES), jnp.float32)
    extended = jnp.concatenate([blank, identity_map], -1)
    output_list, final = run_blocks(terms, value, extended)
    prefix = carried_in(
        (final[..., HEAD_FEATURES:], final[..., :HEAD_FEATURES]),
        "sp",
        compose,
        (identity_map, blank),
    )
    entry_value = prefix[1]
    mixed = output_list[..., :HEAD_FEATURES] + jnp.einsum(
        "apj,ajz->apz", output_list[..., HEAD_FEATURES:], entry_value, precision=highest_precision
    )
    normalized = mixed * lax.rsqrt(jnp.mean(mixed * mixed, -1, keepdims=True) + 1e-06) * head_gain
    gated = (
        (normalized * jax.nn.silu(split_heads(out_gate)))
        .transpose(1, 0, 2)
        .reshape(length, heads * HEAD_FEATURES)
        .astype(jnp.bfloat16)
    )
    split_count = lax.axis_size("tp")
    expert_count = lax.axis_size("sp") * expert_gate.shape[0]
    rows = length // split_count
    first = lax.axis_index("tp") * rows
    projected = lax.psum_scatter(
        jnp.dot(gated, out_weight, preferred_element_type=jnp.float32).astype(jnp.bfloat16),
        "tp",
        scatter_dimension=0,
        tiled=True,
    ).astype(jnp.float32)
    residual = lax.dynamic_slice_in_dim(residual_in, first, rows, 0)
    routes = lax.dynamic_slice_in_dim(expert_index, first, rows, 0)
    weights = lax.dynamic_slice_in_dim(route_weights, first, rows, 0)
    groups = 1
    capacity = 2 * TOP * (length // split_count) // expert_count
    hidden_in = layer_norm(
        residual_scale * residual.astype(jnp.float32) + projected, norm_gain
    ).astype(jnp.bfloat16)
    places = slot_places(routes, groups, capacity, expert_count)
    slots = expert_count * groups * capacity
    table = (places[:, :, None] == jnp.arange(slots, dtype=jnp.int32)).astype(jnp.bfloat16)
    send = jnp.einsum(
        "rs,rd->sd", jnp.sum(table, 1), hidden_in, preferred_element_type=jnp.float32
    ).astype(jnp.bfloat16)
    arrived = lax.all_to_all(
        send.reshape(expert_count, groups * capacity, width),
        "sp",
        split_axis=0,
        concat_axis=0,
        tiled=True,
    ).reshape(slots, width)
    gate_matrix, up_matrix, down_matrix = (expert_gate[0], expert_up[0], expert_down[0])
    piece = lax.all_gather(arrived, "tp", axis=0, tiled=True)
    gate = jnp.dot(piece, gate_matrix, preferred_element_type=jnp.float32)
    up = jnp.dot(piece, up_matrix, preferred_element_type=jnp.float32)
    inner = (jax.nn.silu(gate) * up).astype(jnp.bfloat16)
    partial_value = jnp.dot(inner, down_matrix, preferred_element_type=jnp.float32)
    result = lax.psum_scatter(
        partial_value.astype(jnp.bfloat16), "tp", scatter_dimension=0, tiled=True
    )
    back = lax.all_to_all(
        result.reshape(expert_count, groups * capacity, width),
        "sp",
        split_axis=0,
        concat_axis=0,
        tiled=True,
    ).reshape(slots, width)
    gathered = jnp.einsum("rks,sd->rkd", table, back, preferred_element_type=jnp.float32)
    routed = jnp.sum(weights[..., None] * gathered, 1)
    layer_out = layer_norm(
        residual_scale * hidden_in.astype(jnp.float32) + routed, final_gain
    ).astype(jnp.bfloat16)
    layer_out = lax.all_gather(layer_out, "tp", axis=0, tiled=True)
    return layer_out


def mm(a, b):
    return jnp.dot(a.astype(jnp.bfloat16), b.astype(jnp.bfloat16), preferred_element_type=jnp.float32)


def mm_nt(a, b):
    return lax.dot_general(
        a.astype(jnp.bfloat16),
        b.astype(jnp.bfloat16),
        (((1,), (1,)), ((), ())),
        preferred_element_type=jnp.float32,
    )


def mm_tn(a, b):
    return lax.dot_general(
        a.astype(jnp.bfloat16),
        b.astype(jnp.bfloat16),
        (((0,), (0,)), ((), ())),
        preferred_element_type=jnp.float32,
    )


scope = jax.named_scope


def pick(table, home):
    chosen = []
    for i in range(len(table[0])):
        value = 0
        for h, order in enumerate(table):
            value = value + (home == h).astype(jnp.int32) * order[i]
        chosen.append(value)
    return chosen


def drain(ref, sem):
    pltpu.make_async_copy(ref, ref, sem).wait()


def layer_kernel(
    n_sp,
    n_tp,
    residual_hbm,
    query_hbm,
    key_hbm,
    value_hbm,
    out_gate_hbm,
    beta_hbm,
    decay_hbm,
    decay_log_hbm,
    head_gain_hbm,
    norm_gain_hbm,
    final_gain_hbm,
    index_hbm,
    weights_hbm,
    out_weight_hbm,
    gate_hbm,
    up_hbm,
    down_hbm,
    out_ref,
    residual_ref,
    query_ref,
    key_ref,
    value_ref,
    out_gate_ref,
    beta_ref,
    decay_ref,
    decay_log_ref,
    head_gain_ref,
    norm_gain_ref,
    final_gain_ref,
    index_ref,
    weights_ref,
    out_weight_v,
    gate_v,
    up_v,
    down_v,
    maps_v,
    adds_v,
    state_in,
    state_out,
    mate_out,
    mate_in,
    entry_v,
    mixed_v,
    readout_v,
    gated_v,
    proj_v,
    proj_in,
    hidden_v,
    send_v,
    arrived_v,
    inner_v,
    own_inner_v,
    part_v,
    part_in,
    pair_v,
    result_v,
    back_v,
    final_v,
    local_sem,
    sent_sem,
    state_sem,
    mate_sem,
    entry_sem,
    proj_sem,
    arrive_sem,
    near_sem,
    full_sem,
    pair_sem,
    part_sem,
    back_sem,
    out_sem,
):
    s = lax.axis_index("sp")
    t = lax.axis_index("tp")
    length, width = residual_ref.shape
    heads = beta_ref.shape[0]
    rows = length // n_tp
    chunks, _, group, cap, _ = arrived_v.shape
    half = width // 2
    right, left = slice(half, width), slice(0, half)
    slots = n_sp * cap
    feat = HEAD_FEATURES
    hidden_units = gate_v.shape[1]

    barrier = pltpu.get_barrier_semaphore()
    for k in range(1, n_sp):
        pl.semaphore_signal(
            barrier, inc=1, device_id=(lax.rem(s + k, n_sp), t), device_id_type=MESH
        )
    for k in range(1, n_tp):
        pl.semaphore_signal(
            barrier, inc=1, device_id=(s, lax.rem(t + k, n_tp)), device_id_type=MESH
        )

    pairs = [
        (decay_hbm, decay_ref),
        (decay_log_hbm, decay_log_ref),
        (beta_hbm, beta_ref),
        (key_hbm, key_ref),
        (query_hbm, query_ref),
        (value_hbm, value_ref),
        (out_gate_hbm, out_gate_ref),
        (head_gain_hbm, head_gain_ref),
        (out_weight_hbm, out_weight_v),
        (index_hbm, index_ref),
        (weights_hbm, weights_ref),
        (residual_hbm, residual_ref),
        (norm_gain_hbm, norm_gain_ref),
        (final_gain_hbm, final_gain_ref),
        (gate_hbm.at[0], gate_v),
        (up_hbm.at[0], up_v),
        (down_hbm.at[0], down_v),
    ]
    local = [pltpu.make_async_copy(a, b, local_sem.at[i]) for i, (a, b) in enumerate(pairs)]
    for copy in local:
        copy.start()

    def remote(src, dst, sem_a, sem_b, to_s, to_t):
        return pltpu.make_async_remote_copy(
            src_ref=src,
            dst_ref=dst,
            send_sem=sem_a,
            recv_sem=sem_b,
            device_id=(to_s, to_t),
            device_id_type=MESH,
        )

    with scope("a_load"):
        for copy in local[:6]:
            copy.wait()
    row_id = lax.broadcasted_iota(jnp.int32, (length, length), 0)
    col_id = lax.broadcasted_iota(jnp.int32, (length, length), 1)
    causal = row_id >= col_id
    strict = row_id > col_id
    eye = (row_id == col_id).astype(jnp.float32)
    tril = causal.astype(jnp.float32)
    beta = jax.nn.sigmoid(beta_ref[...].astype(jnp.float32))
    logit = decay_ref[...].astype(jnp.float32)
    soft = jnp.maximum(logit, 0.0) + jnp.log(1.0 + jnp.exp(-jnp.abs(logit)))
    head_eye = lax.broadcasted_iota(jnp.int32, (heads, heads), 0) == lax.broadcasted_iota(
        jnp.int32, (heads, heads), 1
    )
    rate = jnp.sum(jnp.where(head_eye, jnp.exp(decay_log_ref[...]), 0.0), 1, keepdims=True)
    decay = -rate * soft
    exact = functools.partial(
        lax.dot_general, precision=highest_precision, preferred_element_type=jnp.float32
    )
    nt = (((1,), (1,)), ((), ()))
    run_rows = exact(decay, tril, nt)
    run_cols = exact(tril, decay, nt)
    beta_cols = exact(eye, beta, nt)

    lowers, inverses, rights, score_list, q_list, kd_list, last_list = [], [], [], [], [], [], []
    for h in range(heads):
        cols = slice(h * feat, (h + 1) * feat)
        query = unit_rows(query_ref[:, cols].astype(jnp.float32)) * feat ** (-0.5)
        key = unit_rows(key_ref[:, cols].astype(jnp.float32))
        value = value_ref[:, cols].astype(jnp.float32)
        run_c = run_cols[:, h : h + 1]
        run_r = run_rows[h : h + 1, :]
        beta_c = beta_cols[:, h : h + 1]
        last = run_cols[length - 1 : length, h : h + 1]
        within = jnp.where(causal, jnp.exp(jnp.minimum(run_c - run_r, 0.0)), 0.0)
        lowers.append(jnp.where(strict, mm_nt(key, key) * within * beta_c, 0.0))
        score_list.append((mm_nt(query, key) * within).astype(jnp.bfloat16))
        grown = jnp.exp(run_c)
        rights.append(
            jnp.concatenate([value * beta_c, key * (beta_c * grown)], 1).astype(jnp.bfloat16)
        )
        q_list.append(query * grown)
        kd_list.append((key * jnp.exp(last - run_c)).astype(jnp.bfloat16))
        last_list.append(jnp.exp(last))

    def level(size):
        mid = size // 2
        return (row_id // size == col_id // size) & (row_id % size >= mid) & (col_id % size < mid)

    first = level(2)
    inverses = [eye - jnp.where(first, low, 0.0) for low in lowers]
    size = 4
    while size <= length:
        mask = level(size)
        steps = [mm(jnp.where(mask, low, 0.0), inv) for low, inv in zip(lowers, inverses)]
        inverses = [inv - mm(inv, step) for inv, step in zip(inverses, steps)]
        size *= 2
    solved = [mm(inv, right).astype(jnp.bfloat16) for inv, right in zip(inverses, rights)]
    home, core = s // group, s % group
    mate = home * group + (1 - core)
    after = lax.rem(s + group, n_sp)

    def mate_copy(h):
        return remote(
            mate_out.at[h], mate_in.at[h], sent_sem.at[0], mate_sem.at[h], mate, t
        )

    def state_copy(h):
        return remote(
            state_out.at[h], state_in.at[h], sent_sem.at[1], state_sem.at[h], after, t
        )

    def entry_copy(h):
        return remote(
            state_in.at[h], entry_v.at[h], sent_sem.at[2], entry_sem.at[h], mate, t
        )

    for h in range(heads):
        ends = mm_tn(kd_list[h], solved[h])
        adds_v[h] = ends[:, :feat]
        maps = (last_list[h] * eye[:feat, :feat] - ends[:, feat:]).astype(jnp.bfloat16)
        maps_v[h] = maps
        mate_out[h, 0] = maps
        mate_out[h, 1] = ends[:, :feat].astype(jnp.bfloat16)

    with scope("b_barrier"):
        pl.semaphore_wait(barrier, n_sp - 1 + n_tp - 1)

    @pl.when(core == 0)
    def _():
        for h in range(heads):
            mate_copy(h).start()

    for h in range(heads):
        seen = mm(score_list[h], solved[h])
        mixed_v[h] = seen[:, :feat]
        readout_v[h] = (q_list[h] - seen[:, feat:]).astype(jnp.bfloat16)

    @pl.when(core == 1)
    def _():
        for h in range(heads):
            with scope("c_mate"):
                mate_copy(h).wait_recv()

            @pl.when(home == 0)
            def _():
                state_out[h] = (mm(maps_v[h], mate_in[h, 1]) + adds_v[h]).astype(jnp.bfloat16)
                state_copy(h).start()
                entry_v[h] = mate_in[h, 1]

            @pl.when(home > 0)
            def _():
                both = mm(maps_v[h], jnp.concatenate([mate_in[h, 0], mate_in[h, 1]], 1))
                maps_v[h] = both[:, :feat].astype(jnp.bfloat16)
                adds_v[h] = adds_v[h] + both[:, feat:]

        @pl.when(home > 0)
        def _():
            for h in range(heads):
                with scope("c_state"):
                    state_copy(h).wait_recv()

                @pl.when(home < chunks - 1)
                def _():
                    state_out[h] = (mm(maps_v[h], state_in[h]) + adds_v[h]).astype(jnp.bfloat16)
                    state_copy(h).start()

                entry_copy(h).start()

            for h in range(heads):
                entry_v[h] = (
                    mm(mate_in[h, 0], state_in[h]) + mate_in[h, 1].astype(jnp.float32)
                ).astype(jnp.bfloat16)

    @pl.when((core == 0) & (home == 0))
    def _():
        entry_v[...] = jnp.zeros_like(entry_v)

    @pl.when((core == 0) & (home > 0))
    def _():
        for h in range(heads):
            with scope("c_state"):
                entry_copy(h).wait_recv()

    local[6].wait()
    local[7].wait()
    for h in range(heads):
        cols = slice(h * feat, (h + 1) * feat)
        mixed = mixed_v[h] + mm(readout_v[h], entry_v[h])
        normalized = (
            mixed * lax.rsqrt(jnp.mean(mixed * mixed, -1, keepdims=True) + 1e-06) * head_gain_ref[...]
        )
        gate = out_gate_ref[:, cols].astype(jnp.float32)
        gated_v[:, cols] = (normalized * (gate * jax.nn.sigmoid(gate))).astype(jnp.bfloat16)

    local[8].wait()

    def row_block(i):
        return pl.ds(pl.multiple_of(i * rows, rows), rows)

    def project(i, carry):
        cols = pl.ds(pl.multiple_of(i * 512, 512), 512)
        proj_v[:, cols] = jnp.dot(
            gated_v[...], out_weight_v[:, cols], preferred_element_type=jnp.float32
        ).astype(jnp.bfloat16)
        return carry

    for part, cols in enumerate((left, right)):
        steps = half // 512
        with scope("d_project"):
            lax.fori_loop(part * steps, (part + 1) * steps, project, 0)
        for k in range(1, n_tp):
            to = lax.rem(t + k, n_tp)
            copy = remote(
                proj_v.at[row_block(to), cols],
                proj_in.at[k - 1, :, cols],
                sent_sem.at[3],
                proj_sem.at[0],
                s,
                to,
            )
            copy.start()

    for copy in local[9:14]:
        copy.wait()
    own_row = (
        lax.broadcasted_iota(jnp.int32, (rows, length), 1)
        == lax.broadcasted_iota(jnp.int32, (rows, length), 0) + t * rows
    ).astype(jnp.float32)
    index = exact(own_row, index_ref[...].astype(jnp.float32), nt)
    weights = exact(own_row, weights_ref[...], nt)
    slot_id = lax.broadcasted_iota(jnp.int32, (rows, slots), 1)
    owner = (slot_id // cap).astype(jnp.float32)
    picks = [(index[:, j : j + 1] == owner).astype(jnp.float32) for j in range(TOP)]
    both = functools.reduce(jnp.add, picks)
    earlier = (
        lax.broadcasted_iota(jnp.int32, (rows, rows), 0)
        > lax.broadcasted_iota(jnp.int32, (rows, rows), 1)
    ).astype(jnp.float32)
    rank = mm(earlier, both)
    here = (rank == (slot_id % cap).astype(jnp.float32)).astype(jnp.float32)
    tables = [(pick * here).astype(jnp.bfloat16) for pick in picks]
    table = (both * here).astype(jnp.bfloat16)

    tx = t + 1 - 2 * lax.rem(t, 2)
    ty = lax.rem(t + 2, 4)
    td = lax.rem(tx + 2, 4)

    def send_copy(to):
        return remote(
            send_v.at[to], arrived_v.at[home, t, core], sent_sem.at[4], arrive_sem.at[home], to, t
        )

    order = pick(VISITS, home)
    legs = [(home, core, 1), (home, 1 - core, 1)] + [(c, 0, group) for c in order[:-1]]

    def fan_out(j):
        c, low, count = legs[j]
        if j > 0:
            with scope("g_arrive"):
                drain(arrived_v.at[c, t, pl.ds(low, count)], arrive_sem.at[c])

        def one(cols, sem, to):
            mine = arrived_v.at[c, t, pl.ds(low, count), :, cols]
            remote(mine, mine, sent_sem.at[5], sem, s, to).start()

        one(left, near_sem.at[j, 0], tx)
        one(right, near_sem.at[j, 1], ty)
        one(right, full_sem.at[c], tx)
        one(left, full_sem.at[c], ty)

    def relay(j):
        c, low, count = legs[j]
        for i, (near, cols, to) in enumerate(((tx, left, ty), (ty, right, tx))):
            block = arrived_v.at[c, near, pl.ds(low, count), :, cols]
            with scope("h_fan"):
                drain(block, near_sem.at[j, i])
            remote(block, block, sent_sem.at[5], full_sem.at[c], s, to).start()

    def wait_full(k):
        with scope("j_full"):
            drain(arrived_v.at[order[k], pl.ds(0, 2)], full_sem.at[order[k]])

    projected = proj_v[row_block(t), :].astype(jnp.float32)
    with scope("e_proj"):
        drain(proj_in, proj_sem.at[0])
    for k in range(1, n_tp):
        projected = projected + proj_in[k - 1].astype(jnp.float32)
    residual = residual_ref[row_block(t), :].astype(jnp.float32)
    hidden_in = layer_norm(residual_scale * residual + projected, norm_gain_ref[...]).astype(
        jnp.bfloat16
    )
    hidden_v[...] = hidden_in

    send_v[...] = mm_tn(table, hidden_in).astype(jnp.bfloat16).reshape(n_sp, cap, width)

    for i in range(group):

        @pl.when(s != home * group + i)
        def _():
            send_copy(home * group + i).start()

    for there in pick(SENDS, home):
        for i in range(group):
            send_copy(there * group + i).start()

    arrived_v[home, t, core] = send_v[s]

    def part_copy(kind, j):
        src, to = (
            (part_v.at[j, td, :, left], tx),
            (part_v.at[j, td, :, right], ty),
            (part_v.at[j, tx, :, left], tx),
            (part_v.at[j, ty, :, right], ty),
            (pair_v.at[0, j], ty),
            (pair_v.at[1, j], tx),
        )[kind]
        sem = pair_sem.at[j, kind] if kind < 2 else part_sem.at[j, kind % 2]
        return remote(src, part_in.at[kind, j], sent_sem.at[6], sem, s, to)

    def gate_up(j, part, inner):
        piece = arrived_v[order[j]].reshape(n_tp * group * cap, width)
        steps = hidden_units // 256 // 2

        def step(i, carry):
            cols = pl.ds(pl.multiple_of(i * 256, 256), 256)
            gate = jnp.dot(piece, gate_v[:, cols], preferred_element_type=jnp.float32)
            up = jnp.dot(piece, up_v[:, cols], preferred_element_type=jnp.float32)
            inner[:, cols] = (gate * jax.nn.sigmoid(gate) * up).astype(jnp.bfloat16)
            return carry

        with scope("k_gateup"):
            lax.fori_loop(part * steps, (part + 1) * steps, step, 0)

    def down(j, inner, kinds):
        def step(i, carry):
            cols = pl.ds(pl.multiple_of(i * 512, 512), 512)
            part_v[j, :, :, cols] = (
                jnp.dot(
                    inner[...], down_v[:, cols], preferred_element_type=jnp.float32
                )
                .astype(jnp.bfloat16)
                .reshape(n_tp, group * cap, 512)
            )
            return carry

        steps = half // 512
        for part in range(2):
            with scope("l_down"):
                lax.fori_loop(part * steps, (part + 1) * steps, step, 0)
            for kind in range(part, kinds, 2):
                part_copy(kind, j).start()

    def pair_up(j):
        wide = jnp.float32
        for i, (near, cols) in enumerate(((ty, left), (tx, right))):
            with scope("m_pair"):
                drain(part_in.at[i, j], pair_sem.at[j, i])
            pair_v[i, j] = (
                part_v[j, near, :, cols].astype(wide) + part_in[i, j].astype(wide)
            ).astype(jnp.bfloat16)
            part_copy(4 + i, j).start()

    def finish(j):
        for i, cols in enumerate((left, right)):
            with scope("n_finish"):
                drain(part_in.at[pl.ds(0, 2), j], part_sem.at[j, i])
            near = part_in[2 + i, j].astype(jnp.float32)
            far = part_in[4 + i, j].astype(jnp.float32)
            total = part_v[j, t, :, cols].astype(jnp.float32) + near + far
            result_v[j, :, :, cols] = total.astype(jnp.bfloat16).reshape(group, cap, half)
            for m in range(group):
                p = order[j] * group + m

                @pl.when(s != p)
                def _():
                    remote(
                        result_v.at[j, m, :, cols],
                        back_v.at[s, :, cols],
                        sent_sem.at[7],
                        back_sem.at[0],
                        p,
                        t,
                    ).start()

                @pl.when(s == p)
                def _():
                    back_v[s, :, cols] = result_v[j, m, :, cols]

    fan_out(0)
    fan_out(1)

    @pl.when(home == 0)
    def _():
        relay(0)
        relay(1)

    fan_out(2)

    @pl.when(home > 0)
    def _():
        relay(0)
        relay(1)

    for copy in local[14:]:
        copy.wait()
    relay(2)

    @pl.when(home != 1)
    def _():
        fan_out(3)

    own = chunks - 1

    @pl.when(home != 1)
    def _():
        wait_full(own)
        gate_up(own, 0, own_inner_v)

    wait_full(0)
    gate_up(0, 0, inner_v)

    @pl.when(home != 1)
    def _():
        relay(3)
        fan_out(4)

    @pl.when(home == 1)
    def _():
        fan_out(3)

    gate_up(0, 1, inner_v)
    down(0, inner_v, 4)

    @pl.when(home == 1)
    def _():
        wait_full(own)
        gate_up(own, 0, own_inner_v)
        gate_up(own, 1, own_inner_v)
        relay(3)
        fan_out(4)
        down(own, own_inner_v, 4)

    wait_full(1)
    gate_up(1, 0, inner_v)
    relay(4)
    gate_up(1, 1, inner_v)

    @pl.when(home != 1)
    def _():
        gate_up(own, 1, own_inner_v)

    pair_up(0)
    down(1, inner_v, 4)
    wait_full(2)
    gate_up(2, 0, inner_v)
    gate_up(2, 1, inner_v)
    pair_up(1)
    finish(0)
    down(2, inner_v, 4)

    @pl.when(home != 1)
    def _():
        down(own, own_inner_v, 2)

    finish(1)
    pair_up(2)

    @pl.when(home != 1)
    def _():
        part_copy(2, own).start()
        part_copy(3, own).start()

    pair_up(own)
    finish(2)
    finish(own)

    with scope("o_back"):
        drain(back_v.at[pl.ds(0, n_sp - 1)], back_sem.at[0])

    back = back_v[...].reshape(slots, width)
    routed = jnp.zeros((rows, width), jnp.float32)
    for j in range(TOP):
        routed = routed + weights[:, j : j + 1] * mm(tables[j], back)
    final_v[...] = layer_norm(
        residual_scale * hidden_v[...].astype(jnp.float32) + routed, final_gain_ref[...]
    ).astype(jnp.bfloat16)

    def out_copy(owner, q, to, sem):
        cols = pl.ds(q * (width // 4), width // 4)
        cells = out_ref.at[row_block(owner), cols]
        source = final_v.at[:, cols] if owner is t else cells
        return remote(source, cells, sent_sem.at[8], out_sem.at[sem], s, to)

    for q in range(4):
        out_copy(t, q, tx, min(q, 2)).start()
        out_copy(t, 3 - q, ty, min(q, 2) + (3 if q < 2 else 0)).start()
    own_copy = pltpu.make_async_copy(final_v, out_ref.at[row_block(t)], local_sem.at[17])
    own_copy.start()
    piece = final_v.at[:, pl.ds(0, width // 4)]
    with scope("q_out"):
        for q in range(2):
            drain(piece, out_sem.at[q])
            out_copy(tx, q, ty, 2).start()
            drain(piece, out_sem.at[3 + q])
            out_copy(ty, 3 - q, tx, 2).start()

    @pl.when(core == 0)
    def _():
        drain(mate_out, sent_sem.at[0])

    @pl.when((core == 1) & (home < chunks - 1))
    def _():
        drain(state_out, sent_sem.at[1])

    @pl.when((core == 1) & (home > 0))
    def _():
        drain(state_in, sent_sem.at[2])

    drain(proj_in, sent_sem.at[3])
    drain(send_v.at[pl.ds(0, n_sp - 1)], sent_sem.at[4])
    drain(arrived_v.at[:, pl.ds(0, 3)], sent_sem.at[5])
    drain(part_in, sent_sem.at[6])
    drain(back_v.at[pl.ds(0, n_sp - 1)], sent_sem.at[7])
    own_copy.wait()
    with scope("r_out"):
        drain(proj_in.at[pl.ds(0, 2)], out_sem.at[2])
    with scope("s_sends"):
        drain(proj_in, sent_sem.at[8])


def fused(args, n_sp, n_tp, cap):
    (residual_in, queries, keys, values, out_gate, beta_logit, decay_logit, decay_log, head_gain,
     out_weight, norm_gain, final_gain, expert_index, route_weights, expert_gate, expert_up,
     expert_down) = args
    length, width = residual_in.shape
    heads = beta_logit.shape[0]
    rows = length // n_tp
    chunks = n_sp // GROUP
    units = expert_gate.shape[2]
    feat = HEAD_FEATURES
    low, full = jnp.bfloat16, jnp.float32
    hbm = pl.BlockSpec(memory_space=pl.ANY)
    dma = pltpu.SemaphoreType.DMA
    arrays = [
        residual_in, queries, keys, values, out_gate, beta_logit, decay_logit,
        decay_log.reshape(1, heads), head_gain.reshape(1, -1), norm_gain.reshape(1, -1),
        final_gain.reshape(1, -1), expert_index.T, route_weights.T,
    ]
    return pl.pallas_call(
        functools.partial(layer_kernel, n_sp, n_tp),
        out_shape=pltpu.VMEM((length, width), low),
        in_specs=[hbm] * 17,
        out_specs=hbm,
        scratch_shapes=[pltpu.VMEM(a.shape, a.dtype) for a in arrays]
        + [
            pltpu.VMEM(out_weight.shape, low),
            pltpu.VMEM(expert_gate.shape[1:], low),
            pltpu.VMEM(expert_up.shape[1:], low),
            pltpu.VMEM(expert_down.shape[1:], low),
            pltpu.VMEM((heads, feat, feat), low),
            pltpu.VMEM((heads, feat, feat), full),
            pltpu.VMEM((heads, feat, feat), low),
            pltpu.VMEM((heads, feat, feat), low),
            pltpu.VMEM((heads, 2, feat, feat), low),
            pltpu.VMEM((heads, 2, feat, feat), low),
            pltpu.VMEM((heads, feat, feat), low),
            pltpu.VMEM((heads, length, feat), full),
            pltpu.VMEM((heads, length, feat), low),
            pltpu.VMEM((length, heads * feat), low),
            pltpu.VMEM((length, width), low),
            pltpu.VMEM((n_tp - 1, rows, width), low),
            pltpu.VMEM((rows, width), low),
            pltpu.VMEM((n_sp, cap, width), low),
            pltpu.VMEM((chunks, n_tp, GROUP, cap, width), low),
            pltpu.VMEM((n_tp * GROUP * cap, units), low),
            pltpu.VMEM((n_tp * GROUP * cap, units), low),
            pltpu.VMEM((chunks, n_tp, GROUP * cap, width), low),
            pltpu.VMEM((6, chunks, GROUP * cap, width // 2), low),
            pltpu.VMEM((2, chunks, GROUP * cap, width // 2), low),
            pltpu.VMEM((chunks, GROUP, cap, width), low),
            pltpu.VMEM((n_sp, cap, width), low),
            pltpu.VMEM((rows, width), low),
            dma((18,)),
            dma((9,)),
            dma((heads,)),
            dma((heads,)),
            dma((heads,)),
            dma((1,)),
            dma((chunks,)),
            dma((chunks + 1, 2)),
            dma((chunks,)),
            dma((chunks, 2)),
            dma((chunks, 2)),
            dma((1,)),
            dma((5,)),
        ],
        compiler_params=pltpu.CompilerParams(
            collective_id=0, has_side_effects=True, vmem_limit_bytes=60 * 1024 * 1024
        ),
    )(*arrays, out_weight, expert_gate, expert_up, expert_down)


def any_size(*args):
    n_sp, n_tp = lax.axis_size("sp"), lax.axis_size("tp")
    residual_in, expert_gate = args[0], args[14]
    length, width = residual_in.shape
    experts = n_sp * expert_gate.shape[0]
    cap = 2 * TOP * (length // n_tp) // experts
    fits = (
        expert_gate.shape[0] == 1
        and n_sp == GROUP * len(VISITS)
        and n_tp == 4
        and length == HEAD_FEATURES
        and cap % 16 == 0
        and (length // n_tp) % 16 == 0
        and (n_sp * cap) % 128 == 0
        and width % 512 == 0
        and expert_gate.shape[2] % 256 == 0
    )
    return fused(args, n_sp, n_tp, cap) if fits else per_device(*args)


def solution(mesh):
    in_specs = (
        P("sp", None),
        P("sp", "tp"),
        P("sp", "tp"),
        P("sp", "tp"),
        P("sp", "tp"),
        P("tp", "sp"),
        P("tp", "sp"),
        P("tp"),
        P(),
        P("tp", None),
        P(),
        P(),
        P("sp", None),
        P("sp", None),
        P("sp", None, "tp"),
        P("sp", None, "tp"),
        P("sp", "tp", None),
    )
    out_specs = P("sp", None)
    return jax.shard_map(
        any_size, mesh=mesh, in_specs=in_specs, out_specs=out_specs, check_vma=False
    )
```

```python
import functools

import jax
import jax.numpy as jnp
from jax import lax
from jax.experimental import pallas as pl
from jax.experimental.pallas import tpu as pltpu
from jax.sharding import PartitionSpec as P

MESH = pl.DeviceIdType.MESH

HEAD_FEATURES = 128
TOP = 2
BLOCK = 64
GROUP = 2
OUT_PARTS = 8
VISITS = ((1, 2, 3, 0), (0, 3, 2, 1), (0, 3, 1, 2), (0, 1, 2, 3))
SENDS = ((1, 2, 3), (0, 2, 3), (3, 0, 1), (2, 1, 0))


highest_precision = lax.Precision.HIGHEST
residual_scale = 2.0**0.5


def carried_in(x, axis, join, neutral):
    place = lax.axis_index(axis)
    gathered = jax.tree.map(
        lambda a, kind: lax.all_gather(a.astype(kind), axis), x, (jnp.bfloat16, jnp.bfloat16)
    )
    state = jax.tree.map(lambda a, e: jnp.zeros_like(a) + jnp.asarray(e, a.dtype), x, neutral)

    def one(turn, state):
        return join(
            state,
            jax.tree.map(
                lambda a, own: lax.dynamic_index_in_dim(a, turn, 0, False).astype(own.dtype),
                gathered,
                x,
            ),
        )

    return lax.fori_loop(0, place, one, state)


def unit_rows(data):
    return data * lax.rsqrt(jnp.sum(data * data, -1, keepdims=True) + 1e-06)


def layer_norm(data, gain):
    center = data - jnp.mean(data, -1, keepdims=True)
    return center * lax.rsqrt(jnp.mean(center * center, -1, keepdims=True) + 1e-05) * gain


def block_terms(query, key, beta, decay):
    heads, length, width = query.shape
    count = length // BLOCK
    shape = (heads, count, BLOCK, width)
    query = query.reshape(shape)
    key = key.reshape(shape)
    beta = beta.reshape(heads, count, BLOCK)
    running = jnp.cumsum(decay.reshape(heads, count, BLOCK), axis=-1)
    causal = jnp.tril(jnp.ones((BLOCK, BLOCK), bool))
    strict = jnp.tril(jnp.ones((BLOCK, BLOCK), bool), -1)
    within = jnp.exp(jnp.where(causal, running[..., :, None] - running[..., None, :], -jnp.inf))
    key_beta = key * beta[..., None]
    lower = jnp.where(
        strict,
        jnp.einsum("hnid,hnjd->hnij", key_beta, key, precision=highest_precision) * within,
        0.0,
    )
    system = jnp.eye(BLOCK, dtype=jnp.float32) + lower
    weighted = jax.scipy.linalg.solve_triangular(
        system, key_beta * jnp.exp(running)[..., None], lower=True, unit_diagonal=True
    )
    scores = jnp.einsum("hnid,hnjd->hnij", query, key, precision=highest_precision) * within
    query_decayed = query * jnp.exp(running)[..., None]
    key_decayed = key * jnp.exp(running[..., -1:] - running)[..., None]
    block_decay = jnp.exp(running[..., -1])
    return (system, beta, weighted, query_decayed, key_decayed, scores, block_decay)


def run_blocks(terms, value, start):
    system, beta, weighted, query_decayed, key_decayed, scores, block_decay = terms
    heads, count = (beta.shape[0], beta.shape[1])
    fresh = jax.scipy.linalg.solve_triangular(
        system,
        value.reshape(heads, count, BLOCK, -1) * beta[..., None],
        lower=True,
        unit_diagonal=True,
    )
    missing = start.shape[-1] - fresh.shape[-1]
    fresh = jnp.concatenate([fresh, jnp.zeros(fresh.shape[:-1] + (missing,), jnp.float32)], -1)

    def advance(recurrent_state, inputs):
        (
            fresh_value_block,
            block_weighted_values,
            block_queries,
            block_keys,
            block_scores,
            block_decay_factor,
        ) = inputs
        corrected_value = fresh_value_block - jnp.einsum(
            "nya,nag->nyg", block_weighted_values, recurrent_state, precision=highest_precision
        )
        state_next = block_decay_factor[:, None, None] * recurrent_state + jnp.einsum(
            "iyp,iyu->ipu", block_keys, corrected_value, precision=highest_precision
        )
        final_output = jnp.einsum(
            "nya,nag->nyg", block_queries, recurrent_state, precision=highest_precision
        ) + jnp.einsum("emp,epk->emk", block_scores, corrected_value, precision=highest_precision)
        return (state_next, final_output)

    inputs = tuple(
        (
            jnp.moveaxis(item, 1, 0)
            for item in (fresh, weighted, query_decayed, key_decayed, scores, block_decay)
        )
    )
    final, output_list = lax.scan(advance, start, inputs)
    return (jnp.moveaxis(output_list, 0, 1).reshape(heads, count * BLOCK, -1), final)


def compose(earlier, later):
    return (
        jnp.einsum("hij,hjk->hik", later[0], earlier[0], precision=highest_precision),
        jnp.einsum("hij,hjk->hik", later[0], earlier[1], precision=highest_precision) + later[1],
    )


def slot_places(routes, groups, capacity, experts):
    rows, picks = routes.shape
    flat = routes.reshape(groups, rows // groups * picks)
    matches = (flat[..., None] == jnp.arange(experts, dtype=jnp.int32)).astype(jnp.int32)
    before = jnp.cumsum(matches, axis=1) - matches
    rank = jnp.sum(before * matches, -1)
    group = jnp.arange(groups, dtype=jnp.int32)[:, None]
    return ((flat * groups + group) * capacity + rank).reshape(rows, picks)


def per_device(
    residual_in,
    queries,
    keys,
    values,
    out_gate,
    beta_logit,
    decay_logit,
    decay_log,
    head_gain,
    out_weight,
    norm_gain,
    final_gain,
    expert_index,
    route_weights,
    expert_gate,
    expert_up,
    expert_down,
):
    length, width = residual_in.shape
    heads = beta_logit.shape[0]

    def split_heads(data):
        return data.astype(jnp.float32).reshape(length, heads, HEAD_FEATURES).transpose(1, 0, 2)

    query = unit_rows(split_heads(queries)) * HEAD_FEATURES ** (-0.5)
    key = unit_rows(split_heads(keys))
    value = split_heads(values)
    beta = jax.nn.sigmoid(beta_logit.astype(jnp.float32))
    decay = -jnp.exp(decay_log)[:, None] * jax.nn.softplus(decay_logit.astype(jnp.float32))
    terms = block_terms(query, key, beta, decay)
    identity_map = jnp.broadcast_to(
        jnp.eye(HEAD_FEATURES, dtype=jnp.float32), (heads, HEAD_FEATURES, HEAD_FEATURES)
    )
    blank = jnp.zeros((heads, HEAD_FEATURES, HEAD_FEATURES), jnp.float32)
    extended = jnp.concatenate([blank, identity_map], -1)
    output_list, final = run_blocks(terms, value, extended)
    prefix = carried_in(
        (final[..., HEAD_FEATURES:], final[..., :HEAD_FEATURES]),
        "sp",
        compose,
        (identity_map, blank),
    )
    entry_value = prefix[1]
    mixed = output_list[..., :HEAD_FEATURES] + jnp.einsum(
        "apj,ajz->apz", output_list[..., HEAD_FEATURES:], entry_value, precision=highest_precision
    )
    normalized = mixed * lax.rsqrt(jnp.mean(mixed * mixed, -1, keepdims=True) + 1e-06) * head_gain
    gated = (
        (normalized * jax.nn.silu(split_heads(out_gate)))
        .transpose(1, 0, 2)
        .reshape(length, heads * HEAD_FEATURES)
        .astype(jnp.bfloat16)
    )
    split_count = lax.axis_size("tp")
    expert_count = lax.axis_size("sp") * expert_gate.shape[0]
    rows = length // split_count
    first = lax.axis_index("tp") * rows
    projected = lax.psum_scatter(
        jnp.dot(gated, out_weight, preferred_element_type=jnp.float32).astype(jnp.bfloat16),
        "tp",
        scatter_dimension=0,
        tiled=True,
    ).astype(jnp.float32)
    residual = lax.dynamic_slice_in_dim(residual_in, first, rows, 0)
    routes = lax.dynamic_slice_in_dim(expert_index, first, rows, 0)
    weights = lax.dynamic_slice_in_dim(route_weights, first, rows, 0)
    groups = 1
    capacity = 2 * TOP * (length // split_count) // expert_count
    hidden_in = layer_norm(
        residual_scale * residual.astype(jnp.float32) + projected, norm_gain
    ).astype(jnp.bfloat16)
    places = slot_places(routes, groups, capacity, expert_count)
    slots = expert_count * groups * capacity
    table = (places[:, :, None] == jnp.arange(slots, dtype=jnp.int32)).astype(jnp.bfloat16)
    send = jnp.einsum(
        "rs,rd->sd", jnp.sum(table, 1), hidden_in, preferred_element_type=jnp.float32
    ).astype(jnp.bfloat16)
    arrived = lax.all_to_all(
        send.reshape(expert_count, groups * capacity, width),
        "sp",
        split_axis=0,
        concat_axis=0,
        tiled=True,
    ).reshape(slots, width)
    gate_matrix, up_matrix, down_matrix = (expert_gate[0], expert_up[0], expert_down[0])
    piece = lax.all_gather(arrived, "tp", axis=0, tiled=True)
    gate = jnp.dot(piece, gate_matrix, preferred_element_type=jnp.float32)
    up = jnp.dot(piece, up_matrix, preferred_element_type=jnp.float32)
    inner = (jax.nn.silu(gate) * up).astype(jnp.bfloat16)
    partial_value = jnp.dot(inner, down_matrix, preferred_element_type=jnp.float32)
    result = lax.psum_scatter(
        partial_value.astype(jnp.bfloat16), "tp", scatter_dimension=0, tiled=True
    )
    back = lax.all_to_all(
        result.reshape(expert_count, groups * capacity, width),
        "sp",
        split_axis=0,
        concat_axis=0,
        tiled=True,
    ).reshape(slots, width)
    gathered = jnp.einsum("rks,sd->rkd", table, back, preferred_element_type=jnp.float32)
    routed = jnp.sum(weights[..., None] * gathered, 1)
    layer_out = layer_norm(
        residual_scale * hidden_in.astype(jnp.float32) + routed, final_gain
    ).astype(jnp.bfloat16)
    layer_out = lax.all_gather(layer_out, "tp", axis=0, tiled=True)
    return layer_out


def mm(a, b):
    return jnp.dot(a.astype(jnp.bfloat16), b.astype(jnp.bfloat16), preferred_element_type=jnp.float32)


def mm_nt(a, b):
    return lax.dot_general(
        a.astype(jnp.bfloat16),
        b.astype(jnp.bfloat16),
        (((1,), (1,)), ((), ())),
        preferred_element_type=jnp.float32,
    )


def mm_tn(a, b):
    return lax.dot_general(
        a.astype(jnp.bfloat16),
        b.astype(jnp.bfloat16),
        (((0,), (0,)), ((), ())),
        preferred_element_type=jnp.float32,
    )


scope = jax.named_scope


def pick(table, home):
    chosen = []
    for i in range(len(table[0])):
        value = 0
        for h, order in enumerate(table):
            value = value + (home == h).astype(jnp.int32) * order[i]
        chosen.append(value)
    return chosen


def drain(ref, sem):
    pltpu.make_async_copy(ref, ref, sem).wait()


def layer_kernel(
    n_sp,
    n_tp,
    residual_hbm,
    query_hbm,
    key_hbm,
    value_hbm,
    out_gate_hbm,
    beta_hbm,
    decay_hbm,
    decay_log_hbm,
    head_gain_hbm,
    norm_gain_hbm,
    final_gain_hbm,
    index_hbm,
    weights_hbm,
    out_weight_hbm,
    gate_hbm,
    up_hbm,
    down_hbm,
    out_ref,
    residual_ref,
    query_ref,
    key_ref,
    value_ref,
    out_gate_ref,
    beta_ref,
    decay_ref,
    decay_log_ref,
    head_gain_ref,
    norm_gain_ref,
    final_gain_ref,
    index_ref,
    weights_ref,
    out_weight_v,
    gate_v,
    up_v,
    down_v,
    maps_v,
    adds_v,
    state_in,
    state_out,
    mate_out,
    mate_in,
    entry_v,
    mixed_v,
    readout_v,
    gated_v,
    proj_v,
    proj_in,
    hidden_v,
    send_v,
    arrived_v,
    inner_v,
    own_inner_v,
    part_v,
    part_in,
    pair_v,
    result_v,
    back_v,
    final_v,
    local_sem,
    sent_sem,
    state_sem,
    mate_sem,
    entry_sem,
    proj_sem,
    arrive_sem,
    near_sem,
    full_sem,
    pair_sem,
    part_sem,
    back_sem,
    out_sem,
):
    s = lax.axis_index("sp")
    t = lax.axis_index("tp")
    length, width = residual_ref.shape
    heads = beta_ref.shape[0]
    rows = length // n_tp
    chunks, _, group, cap, _ = arrived_v.shape
    half = width // 2
    right, left = slice(half, width), slice(0, half)
    slots = n_sp * cap
    feat = HEAD_FEATURES
    hidden_units = gate_v.shape[1]

    barrier = pltpu.get_barrier_semaphore()
    for k in range(1, n_sp):
        pl.semaphore_signal(
            barrier, inc=1, device_id=(lax.rem(s + k, n_sp), t), device_id_type=MESH
        )
    for k in range(1, n_tp):
        pl.semaphore_signal(
            barrier, inc=1, device_id=(s, lax.rem(t + k, n_tp)), device_id_type=MESH
        )

    pairs = [
        (decay_hbm, decay_ref),
        (decay_log_hbm, decay_log_ref),
        (beta_hbm, beta_ref),
        (key_hbm, key_ref),
        (query_hbm, query_ref),
        (value_hbm, value_ref),
        (out_gate_hbm, out_gate_ref),
        (head_gain_hbm, head_gain_ref),
        (out_weight_hbm, out_weight_v),
        (index_hbm, index_ref),
        (weights_hbm, weights_ref),
        (residual_hbm, residual_ref),
        (norm_gain_hbm, norm_gain_ref),
        (final_gain_hbm, final_gain_ref),
        (gate_hbm.at[0], gate_v),
        (up_hbm.at[0], up_v),
        (down_hbm.at[0], down_v),
    ]
    local = [pltpu.make_async_copy(a, b, local_sem.at[i]) for i, (a, b) in enumerate(pairs)]
    for copy in local:
        copy.start()

    def remote(src, dst, sem_a, sem_b, to_s, to_t):
        return pltpu.make_async_remote_copy(
            src_ref=src,
            dst_ref=dst,
            send_sem=sem_a,
            recv_sem=sem_b,
            device_id=(to_s, to_t),
            device_id_type=MESH,
        )

    with scope("a_load"):
        for copy in local[:6]:
            copy.wait()
    row_id = lax.broadcasted_iota(jnp.int32, (length, length), 0)
    col_id = lax.broadcasted_iota(jnp.int32, (length, length), 1)
    causal = row_id >= col_id
    strict = row_id > col_id
    eye = (row_id == col_id).astype(jnp.float32)
    tril = causal.astype(jnp.float32)
    beta = jax.nn.sigmoid(beta_ref[...].astype(jnp.float32))
    logit = decay_ref[...].astype(jnp.float32)
    soft = jnp.maximum(logit, 0.0) + jnp.log(1.0 + jnp.exp(-jnp.abs(logit)))
    head_eye = lax.broadcasted_iota(jnp.int32, (heads, heads), 0) == lax.broadcasted_iota(
        jnp.int32, (heads, heads), 1
    )
    rate = jnp.sum(jnp.where(head_eye, jnp.exp(decay_log_ref[...]), 0.0), 1, keepdims=True)
    decay = -rate * soft
    exact = functools.partial(
        lax.dot_general, precision=highest_precision, preferred_element_type=jnp.float32
    )
    nt = (((1,), (1,)), ((), ()))
    run_rows = exact(decay, tril, nt)
    run_cols = exact(tril, decay, nt)
    beta_cols = exact(eye, beta, nt)

    lowers, inverses, rights, score_list, q_list, kd_list, last_list = [], [], [], [], [], [], []
    for h in range(heads):
        cols = slice(h * feat, (h + 1) * feat)
        query = unit_rows(query_ref[:, cols].astype(jnp.float32)) * feat ** (-0.5)
        key = unit_rows(key_ref[:, cols].astype(jnp.float32))
        value = value_ref[:, cols].astype(jnp.float32)
        run_c = run_cols[:, h : h + 1]
        run_r = run_rows[h : h + 1, :]
        beta_c = beta_cols[:, h : h + 1]
        last = run_cols[length - 1 : length, h : h + 1]
        within = jnp.where(causal, jnp.exp(jnp.minimum(run_c - run_r, 0.0)), 0.0)
        lowers.append(jnp.where(strict, mm_nt(key, key) * within * beta_c, 0.0))
        score_list.append((mm_nt(query, key) * within).astype(jnp.bfloat16))
        grown = jnp.exp(run_c)
        rights.append(
            jnp.concatenate([value * beta_c, key * (beta_c * grown)], 1).astype(jnp.bfloat16)
        )
        q_list.append(query * grown)
        kd_list.append((key * jnp.exp(last - run_c)).astype(jnp.bfloat16))
        last_list.append(jnp.exp(last))

    def level(size):
        mid = size // 2
        return (row_id // size == col_id // size) & (row_id % size >= mid) & (col_id % size < mid)

    first = level(2)
    inverses = [eye - jnp.where(first, low, 0.0) for low in lowers]
    size = 4
    while size <= length:
        mask = level(size)
        steps = [mm(jnp.where(mask, low, 0.0), inv) for low, inv in zip(lowers, inverses)]
        inverses = [inv - mm(inv, step) for inv, step in zip(inverses, steps)]
        size *= 2
    solved = [mm(inv, right).astype(jnp.bfloat16) for inv, right in zip(inverses, rights)]
    home, core = s // group, s % group
    mate = home * group + (1 - core)
    after = lax.rem(s + group, n_sp)

    def mate_copy(h):
        return remote(
            mate_out.at[h], mate_in.at[h], sent_sem.at[0], mate_sem.at[h], mate, t
        )

    def state_copy(h):
        return remote(
            state_out.at[h], state_in.at[h], sent_sem.at[1], state_sem.at[h], after, t
        )

    def entry_copy(h):
        return remote(
            state_in.at[h], entry_v.at[h], sent_sem.at[2], entry_sem.at[h], mate, t
        )

    for h in range(heads):
        ends = mm_tn(kd_list[h], solved[h])
        adds_v[h] = ends[:, :feat]
        maps = (last_list[h] * eye[:feat, :feat] - ends[:, feat:]).astype(jnp.bfloat16)
        maps_v[h] = maps
        mate_out[h, 0] = maps
        mate_out[h, 1] = ends[:, :feat].astype(jnp.bfloat16)

    with scope("b_barrier"):
        pl.semaphore_wait(barrier, n_sp - 1 + n_tp - 1)

    @pl.when(core == 0)
    def _():
        for h in range(heads):
            mate_copy(h).start()

    for h in range(heads):
        seen = mm(score_list[h], solved[h])
        mixed_v[h] = seen[:, :feat]
        readout_v[h] = (q_list[h] - seen[:, feat:]).astype(jnp.bfloat16)

    @pl.when(core == 1)
    def _():
        for h in range(heads):
            with scope("c_mate"):
                mate_copy(h).wait_recv()

            @pl.when(home == 0)
            def _():
                state_out[h] = (mm(maps_v[h], mate_in[h, 1]) + adds_v[h]).astype(jnp.bfloat16)
                state_copy(h).start()
                entry_v[h] = mate_in[h, 1]

            @pl.when(home > 0)
            def _():
                both = mm(maps_v[h], jnp.concatenate([mate_in[h, 0], mate_in[h, 1]], 1))
                maps_v[h] = both[:, :feat].astype(jnp.bfloat16)
                adds_v[h] = adds_v[h] + both[:, feat:]

        @pl.when(home > 0)
        def _():
            for h in range(heads):
                with scope("c_state"):
                    state_copy(h).wait_recv()

                @pl.when(home < chunks - 1)
                def _():
                    state_out[h] = (mm(maps_v[h], state_in[h]) + adds_v[h]).astype(jnp.bfloat16)
                    state_copy(h).start()

                entry_copy(h).start()

            for h in range(heads):
                entry_v[h] = (
                    mm(mate_in[h, 0], state_in[h]) + mate_in[h, 1].astype(jnp.float32)
                ).astype(jnp.bfloat16)

    @pl.when((core == 0) & (home == 0))
    def _():
        entry_v[...] = jnp.zeros_like(entry_v)

    @pl.when((core == 0) & (home > 0))
    def _():
        for h in range(heads):
            with scope("c_state"):
                entry_copy(h).wait_recv()

    local[6].wait()
    local[7].wait()
    for h in range(heads):
        cols = slice(h * feat, (h + 1) * feat)
        mixed = mixed_v[h] + mm(readout_v[h], entry_v[h])
        normalized = (
            mixed * lax.rsqrt(jnp.mean(mixed * mixed, -1, keepdims=True) + 1e-06) * head_gain_ref[...]
        )
        gate = out_gate_ref[:, cols].astype(jnp.float32)
        gated_v[:, cols] = (normalized * (gate * jax.nn.sigmoid(gate))).astype(jnp.bfloat16)

    local[8].wait()

    def row_block(i):
        return pl.ds(pl.multiple_of(i * rows, rows), rows)

    def project(i, carry):
        cols = pl.ds(pl.multiple_of(i * 512, 512), 512)
        proj_v[:, cols] = jnp.dot(
            gated_v[...], out_weight_v[:, cols], preferred_element_type=jnp.float32
        ).astype(jnp.bfloat16)
        return carry

    for part, cols in enumerate((left, right)):
        steps = half // 512
        with scope("d_project"):
            lax.fori_loop(part * steps, (part + 1) * steps, project, 0)
        for k in range(1, n_tp):
            to = lax.rem(t + k, n_tp)
            copy = remote(
                proj_v.at[row_block(to), cols],
                proj_in.at[k - 1, :, cols],
                sent_sem.at[3],
                proj_sem.at[0],
                s,
                to,
            )
            copy.start()

    for copy in local[9:14]:
        copy.wait()
    own_row = (
        lax.broadcasted_iota(jnp.int32, (rows, length), 1)
        == lax.broadcasted_iota(jnp.int32, (rows, length), 0) + t * rows
    ).astype(jnp.float32)
    index = exact(own_row, index_ref[...].astype(jnp.float32), nt)
    weights = exact(own_row, weights_ref[...], nt)
    slot_id = lax.broadcasted_iota(jnp.int32, (rows, slots), 1)
    owner = (slot_id // cap).astype(jnp.float32)
    picks = [(index[:, j : j + 1] == owner).astype(jnp.float32) for j in range(TOP)]
    both = functools.reduce(jnp.add, picks)
    earlier = (
        lax.broadcasted_iota(jnp.int32, (rows, rows), 0)
        > lax.broadcasted_iota(jnp.int32, (rows, rows), 1)
    ).astype(jnp.float32)
    rank = mm(earlier, both)
    here = (rank == (slot_id % cap).astype(jnp.float32)).astype(jnp.float32)
    tables = [(pick * here).astype(jnp.bfloat16) for pick in picks]
    table = (both * here).astype(jnp.bfloat16)

    tx = t + 1 - 2 * lax.rem(t, 2)
    ty = lax.rem(t + 2, 4)
    td = lax.rem(tx + 2, 4)

    def send_copy(to):
        return remote(
            send_v.at[to], arrived_v.at[home, t, core], sent_sem.at[4], arrive_sem.at[home], to, t
        )

    order = pick(VISITS, home)
    legs = [(home, core, 1), (home, 1 - core, 1)] + [(c, 0, group) for c in order[:-1]]

    def fan_out(j):
        c, low, count = legs[j]
        if j > 0:
            with scope("g_arrive"):
                drain(arrived_v.at[c, t, pl.ds(low, count)], arrive_sem.at[c])

        def one(cols, sem, to):
            mine = arrived_v.at[c, t, pl.ds(low, count), :, cols]
            remote(mine, mine, sent_sem.at[5], sem, s, to).start()

        one(left, near_sem.at[j, 0], tx)
        one(right, near_sem.at[j, 1], ty)
        one(right, full_sem.at[c], tx)
        one(left, full_sem.at[c], ty)

    def relay(j):
        c, low, count = legs[j]
        for i, (near, cols, to) in enumerate(((tx, left, ty), (ty, right, tx))):
            block = arrived_v.at[c, near, pl.ds(low, count), :, cols]
            with scope("h_fan"):
                drain(block, near_sem.at[j, i])
            remote(block, block, sent_sem.at[5], full_sem.at[c], s, to).start()

    def wait_full(k):
        with scope("j_full"):
            drain(arrived_v.at[order[k], pl.ds(0, 2)], full_sem.at[order[k]])

    projected = proj_v[row_block(t), :].astype(jnp.float32)
    with scope("e_proj"):
        drain(proj_in, proj_sem.at[0])
    for k in range(1, n_tp):
        projected = projected + proj_in[k - 1].astype(jnp.float32)
    residual = residual_ref[row_block(t), :].astype(jnp.float32)
    hidden_in = layer_norm(residual_scale * residual + projected, norm_gain_ref[...]).astype(
        jnp.bfloat16
    )
    hidden_v[...] = hidden_in

    send_v[...] = mm_tn(table, hidden_in).astype(jnp.bfloat16).reshape(n_sp, cap, width)

    for i in range(group):

        @pl.when(s != home * group + i)
        def _():
            send_copy(home * group + i).start()

    for there in pick(SENDS, home):
        for i in range(group):
            send_copy(there * group + i).start()

    arrived_v[home, t, core] = send_v[s]

    def part_copy(kind, j):
        src, to = (
            (part_v.at[j, td, :, left], tx),
            (part_v.at[j, td, :, right], ty),
            (part_v.at[j, tx, :, left], tx),
            (part_v.at[j, ty, :, right], ty),
            (pair_v.at[0, j], ty),
            (pair_v.at[1, j], tx),
        )[kind]
        sem = pair_sem.at[j, kind] if kind < 2 else part_sem.at[j, kind % 2]
        return remote(src, part_in.at[kind, j], sent_sem.at[6], sem, s, to)

    def gate_up(j, part, inner):
        piece = arrived_v[order[j]].reshape(n_tp * group * cap, width)
        steps = hidden_units // 256 // 2

        def step(i, carry):
            cols = pl.ds(pl.multiple_of(i * 256, 256), 256)
            gate = jnp.dot(piece, gate_v[:, cols], preferred_element_type=jnp.float32)
            up = jnp.dot(piece, up_v[:, cols], preferred_element_type=jnp.float32)
            inner[:, cols] = (gate * jax.nn.sigmoid(gate) * up).astype(jnp.bfloat16)
            return carry

        with scope("k_gateup"):
            lax.fori_loop(part * steps, (part + 1) * steps, step, 0)

    def down(j, inner, kinds):
        def step(i, carry):
            cols = pl.ds(pl.multiple_of(i * 512, 512), 512)
            part_v[j, :, :, cols] = (
                jnp.dot(
                    inner[...], down_v[:, cols], preferred_element_type=jnp.float32
                )
                .astype(jnp.bfloat16)
                .reshape(n_tp, group * cap, 512)
            )
            return carry

        steps = half // 512
        for part in range(2):
            with scope("l_down"):
                lax.fori_loop(part * steps, (part + 1) * steps, step, 0)
            for kind in range(part, kinds, 2):
                part_copy(kind, j).start()

    def pair_up(j):
        wide = jnp.float32
        for i, (near, cols) in enumerate(((ty, left), (tx, right))):
            with scope("m_pair"):
                drain(part_in.at[i, j], pair_sem.at[j, i])
            pair_v[i, j] = (
                part_v[j, near, :, cols].astype(wide) + part_in[i, j].astype(wide)
            ).astype(jnp.bfloat16)
            part_copy(4 + i, j).start()

    def finish(j):
        for i, cols in enumerate((left, right)):
            with scope("n_finish"):
                drain(part_in.at[pl.ds(0, 2), j], part_sem.at[j, i])
            near = part_in[2 + i, j].astype(jnp.float32)
            far = part_in[4 + i, j].astype(jnp.float32)
            total = part_v[j, t, :, cols].astype(jnp.float32) + near + far
            result_v[j, :, :, cols] = total.astype(jnp.bfloat16).reshape(group, cap, half)
            for m in range(group):
                p = order[j] * group + m

                @pl.when(s != p)
                def _():
                    remote(
                        result_v.at[j, m, :, cols],
                        back_v.at[s, :, cols],
                        sent_sem.at[7],
                        back_sem.at[0],
                        p,
                        t,
                    ).start()

                @pl.when(s == p)
                def _():
                    back_v[s, :, cols] = result_v[j, m, :, cols]

    fan_out(0)
    fan_out(1)

    @pl.when(home == 0)
    def _():
        relay(0)
        relay(1)

    fan_out(2)

    @pl.when(home > 0)
    def _():
        relay(0)
        relay(1)

    for copy in local[14:]:
        copy.wait()
    relay(2)

    @pl.when(home != 1)
    def _():
        fan_out(3)

    own = chunks - 1

    @pl.when(home != 1)
    def _():
        wait_full(own)
        gate_up(own, 0, own_inner_v)

    wait_full(0)
    gate_up(0, 0, inner_v)

    @pl.when(home != 1)
    def _():
        relay(3)
        fan_out(4)

    @pl.when(home == 1)
    def _():
        fan_out(3)

    gate_up(0, 1, inner_v)
    down(0, inner_v, 4)

    @pl.when(home == 1)
    def _():
        wait_full(own)
        gate_up(own, 0, own_inner_v)
        gate_up(own, 1, own_inner_v)
        relay(3)
        fan_out(4)
        down(own, own_inner_v, 0)

    wait_full(1)
    gate_up(1, 0, inner_v)
    relay(4)
    gate_up(1, 1, inner_v)

    @pl.when(home != 1)
    def _():
        gate_up(own, 1, own_inner_v)

    pair_up(0)
    down(1, inner_v, 4)
    wait_full(2)
    gate_up(2, 0, inner_v)
    gate_up(2, 1, inner_v)
    pair_up(1)
    finish(0)
    down(2, inner_v, 4)

    @pl.when(home == 1)
    def _():
        part_copy(0, own).start()
        part_copy(1, own).start()

    @pl.when(home != 1)
    def _():
        down(own, own_inner_v, 2)

    finish(1)
    pair_up(2)

    part_copy(2, own).start()
    part_copy(3, own).start()
    pair_up(own)
    finish(2)
    finish(own)

    with scope("o_back"):
        drain(back_v.at[pl.ds(0, n_sp - 1)], back_sem.at[0])

    back = back_v[...].reshape(slots, width)
    chosen = mm(jnp.concatenate(tables, 0), back)
    routed = jnp.zeros((rows, width), jnp.float32)
    for j in range(TOP):
        routed = routed + weights[:, j : j + 1] * chosen[j * rows : (j + 1) * rows]
    final_v[...] = layer_norm(
        residual_scale * hidden_v[...].astype(jnp.float32) + routed, final_gain_ref[...]
    ).astype(jnp.bfloat16)

    def out_copy(owner, q, to, sem):
        cols = pl.ds(q * (width // OUT_PARTS), width // OUT_PARTS)
        cells = out_ref.at[row_block(owner), cols]
        source = final_v.at[:, cols] if owner is t else cells
        return remote(source, cells, sent_sem.at[8], out_sem.at[sem], s, to)

    early = OUT_PARTS // 2
    for q in range(OUT_PARTS):
        rest = 2 * early
        out_copy(t, q, tx, q if q < early else rest).start()
        out_copy(t, OUT_PARTS - 1 - q, ty, early + q if q < early else rest).start()
    own_copy = pltpu.make_async_copy(final_v, out_ref.at[row_block(t)], local_sem.at[17])
    own_copy.start()
    piece = final_v.at[:, pl.ds(0, width // OUT_PARTS)]
    with scope("q_out"):
        for q in range(early):
            drain(piece, out_sem.at[q])
            out_copy(tx, q, ty, 2 * early).start()
            drain(piece, out_sem.at[early + q])
            out_copy(ty, OUT_PARTS - 1 - q, tx, 2 * early).start()

    @pl.when(core == 0)
    def _():
        drain(mate_out, sent_sem.at[0])

    @pl.when((core == 1) & (home < chunks - 1))
    def _():
        drain(state_out, sent_sem.at[1])

    @pl.when((core == 1) & (home > 0))
    def _():
        drain(state_in, sent_sem.at[2])

    drain(proj_in, sent_sem.at[3])
    drain(send_v.at[pl.ds(0, n_sp - 1)], sent_sem.at[4])
    drain(arrived_v.at[:, pl.ds(0, 3)], sent_sem.at[5])
    drain(part_in, sent_sem.at[6])
    drain(back_v.at[pl.ds(0, n_sp - 1)], sent_sem.at[7])
    own_copy.wait()
    with scope("r_out"):
        drain(proj_in.at[pl.ds(0, 2)], out_sem.at[OUT_PARTS])
    with scope("s_sends"):
        drain(proj_in, sent_sem.at[8])


def fused(args, n_sp, n_tp, cap):
    (residual_in, queries, keys, values, out_gate, beta_logit, decay_logit, decay_log, head_gain,
     out_weight, norm_gain, final_gain, expert_index, route_weights, expert_gate, expert_up,
     expert_down) = args
    length, width = residual_in.shape
    heads = beta_logit.shape[0]
    rows = length // n_tp
    chunks = n_sp // GROUP
    units = expert_gate.shape[2]
    feat = HEAD_FEATURES
    low, full = jnp.bfloat16, jnp.float32
    hbm = pl.BlockSpec(memory_space=pl.ANY)
    dma = pltpu.SemaphoreType.DMA
    arrays = [
        residual_in, queries, keys, values, out_gate, beta_logit, decay_logit,
        decay_log.reshape(1, heads), head_gain.reshape(1, -1), norm_gain.reshape(1, -1),
        final_gain.reshape(1, -1), expert_index.T, route_weights.T,
    ]
    return pl.pallas_call(
        functools.partial(layer_kernel, n_sp, n_tp),
        out_shape=pltpu.VMEM((length, width), low),
        in_specs=[hbm] * 17,
        out_specs=hbm,
        scratch_shapes=[pltpu.VMEM(a.shape, a.dtype) for a in arrays]
        + [
            pltpu.VMEM(out_weight.shape, low),
            pltpu.VMEM(expert_gate.shape[1:], low),
            pltpu.VMEM(expert_up.shape[1:], low),
            pltpu.VMEM(expert_down.shape[1:], low),
            pltpu.VMEM((heads, feat, feat), low),
            pltpu.VMEM((heads, feat, feat), full),
            pltpu.VMEM((heads, feat, feat), low),
            pltpu.VMEM((heads, feat, feat), low),
            pltpu.VMEM((heads, 2, feat, feat), low),
            pltpu.VMEM((heads, 2, feat, feat), low),
            pltpu.VMEM((heads, feat, feat), low),
            pltpu.VMEM((heads, length, feat), full),
            pltpu.VMEM((heads, length, feat), low),
            pltpu.VMEM((length, heads * feat), low),
            pltpu.VMEM((length, width), low),
            pltpu.VMEM((n_tp - 1, rows, width), low),
            pltpu.VMEM((rows, width), low),
            pltpu.VMEM((n_sp, cap, width), low),
            pltpu.VMEM((chunks, n_tp, GROUP, cap, width), low),
            pltpu.VMEM((n_tp * GROUP * cap, units), low),
            pltpu.VMEM((n_tp * GROUP * cap, units), low),
            pltpu.VMEM((chunks, n_tp, GROUP * cap, width), low),
            pltpu.VMEM((6, chunks, GROUP * cap, width // 2), low),
            pltpu.VMEM((2, chunks, GROUP * cap, width // 2), low),
            pltpu.VMEM((chunks, GROUP, cap, width), low),
            pltpu.VMEM((n_sp, cap, width), low),
            pltpu.VMEM((rows, width), low),
            dma((18,)),
            dma((9,)),
            dma((heads,)),
            dma((heads,)),
            dma((heads,)),
            dma((1,)),
            dma((chunks,)),
            dma((chunks + 1, 2)),
            dma((chunks,)),
            dma((chunks, 2)),
            dma((chunks, 2)),
            dma((1,)),
            dma((OUT_PARTS + 1,)),
        ],
        compiler_params=pltpu.CompilerParams(
            collective_id=0, has_side_effects=True, vmem_limit_bytes=60 * 1024 * 1024
        ),
    )(*arrays, out_weight, expert_gate, expert_up, expert_down)


def any_size(*args):
    n_sp, n_tp = lax.axis_size("sp"), lax.axis_size("tp")
    residual_in, expert_gate = args[0], args[14]
    length, width = residual_in.shape
    experts = n_sp * expert_gate.shape[0]
    cap = 2 * TOP * (length // n_tp) // experts
    fits = (
        expert_gate.shape[0] == 1
        and n_sp == GROUP * len(VISITS)
        and n_tp == 4
        and length == HEAD_FEATURES
        and cap % 16 == 0
        and (length // n_tp) % 16 == 0
        and (n_sp * cap) % 128 == 0
        and width % 1024 == 0
        and width % (128 * OUT_PARTS) == 0
        and expert_gate.shape[2] % 256 == 0
    )
    return fused(args, n_sp, n_tp, cap) if fits else per_device(*args)


def solution(mesh):
    in_specs = (
        P("sp", None),
        P("sp", "tp"),
        P("sp", "tp"),
        P("sp", "tp"),
        P("sp", "tp"),
        P("tp", "sp"),
        P("tp", "sp"),
        P("tp"),
        P(),
        P("tp", None),
        P(),
        P(),
        P("sp", None),
        P("sp", None),
        P("sp", None, "tp"),
        P("sp", None, "tp"),
        P("sp", "tp", None),
    )
    out_specs = P("sp", None)
    return jax.shard_map(
        any_size, mesh=mesh, in_specs=in_specs, out_specs=out_specs, check_vma=False
    )
```

```python
import functools

import jax
import jax.numpy as jnp
from jax import lax
from jax.experimental import pallas as pl
from jax.experimental.pallas import tpu as pltpu
from jax.sharding import PartitionSpec as P

MESH = pl.DeviceIdType.MESH

HEAD_FEATURES = 128
TOP = 2
BLOCK = 64
GROUP = 2
OUT_PARTS = 8
VISITS = ((1, 2, 3, 0), (0, 3, 2, 1), (0, 3, 1, 2), (0, 1, 2, 3))
SENDS = ((1, 2, 3), (0, 2, 3), (3, 0, 1), (2, 1, 0))


highest_precision = lax.Precision.HIGHEST
residual_scale = 2.0**0.5


def carried_in(x, axis, join, neutral):
    place = lax.axis_index(axis)
    gathered = jax.tree.map(
        lambda a, kind: lax.all_gather(a.astype(kind), axis), x, (jnp.bfloat16, jnp.bfloat16)
    )
    state = jax.tree.map(lambda a, e: jnp.zeros_like(a) + jnp.asarray(e, a.dtype), x, neutral)

    def one(turn, state):
        return join(
            state,
            jax.tree.map(
                lambda a, own: lax.dynamic_index_in_dim(a, turn, 0, False).astype(own.dtype),
                gathered,
                x,
            ),
        )

    return lax.fori_loop(0, place, one, state)


def unit_rows(data):
    return data * lax.rsqrt(jnp.sum(data * data, -1, keepdims=True) + 1e-06)


def layer_norm(data, gain):
    center = data - jnp.mean(data, -1, keepdims=True)
    return center * lax.rsqrt(jnp.mean(center * center, -1, keepdims=True) + 1e-05) * gain


def block_terms(query, key, beta, decay):
    heads, length, width = query.shape
    count = length // BLOCK
    shape = (heads, count, BLOCK, width)
    query = query.reshape(shape)
    key = key.reshape(shape)
    beta = beta.reshape(heads, count, BLOCK)
    running = jnp.cumsum(decay.reshape(heads, count, BLOCK), axis=-1)
    causal = jnp.tril(jnp.ones((BLOCK, BLOCK), bool))
    strict = jnp.tril(jnp.ones((BLOCK, BLOCK), bool), -1)
    within = jnp.exp(jnp.where(causal, running[..., :, None] - running[..., None, :], -jnp.inf))
    key_beta = key * beta[..., None]
    lower = jnp.where(
        strict,
        jnp.einsum("hnid,hnjd->hnij", key_beta, key, precision=highest_precision) * within,
        0.0,
    )
    system = jnp.eye(BLOCK, dtype=jnp.float32) + lower
    weighted = jax.scipy.linalg.solve_triangular(
        system, key_beta * jnp.exp(running)[..., None], lower=True, unit_diagonal=True
    )
    scores = jnp.einsum("hnid,hnjd->hnij", query, key, precision=highest_precision) * within
    query_decayed = query * jnp.exp(running)[..., None]
    key_decayed = key * jnp.exp(running[..., -1:] - running)[..., None]
    block_decay = jnp.exp(running[..., -1])
    return (system, beta, weighted, query_decayed, key_decayed, scores, block_decay)


def run_blocks(terms, value, start):
    system, beta, weighted, query_decayed, key_decayed, scores, block_decay = terms
    heads, count = (beta.shape[0], beta.shape[1])
    fresh = jax.scipy.linalg.solve_triangular(
        system,
        value.reshape(heads, count, BLOCK, -1) * beta[..., None],
        lower=True,
        unit_diagonal=True,
    )
    missing = start.shape[-1] - fresh.shape[-1]
    fresh = jnp.concatenate([fresh, jnp.zeros(fresh.shape[:-1] + (missing,), jnp.float32)], -1)

    def advance(recurrent_state, inputs):
        (
            fresh_value_block,
            block_weighted_values,
            block_queries,
            block_keys,
            block_scores,
            block_decay_factor,
        ) = inputs
        corrected_value = fresh_value_block - jnp.einsum(
            "nya,nag->nyg", block_weighted_values, recurrent_state, precision=highest_precision
        )
        state_next = block_decay_factor[:, None, None] * recurrent_state + jnp.einsum(
            "iyp,iyu->ipu", block_keys, corrected_value, precision=highest_precision
        )
        final_output = jnp.einsum(
            "nya,nag->nyg", block_queries, recurrent_state, precision=highest_precision
        ) + jnp.einsum("emp,epk->emk", block_scores, corrected_value, precision=highest_precision)
        return (state_next, final_output)

    inputs = tuple(
        (
            jnp.moveaxis(item, 1, 0)
            for item in (fresh, weighted, query_decayed, key_decayed, scores, block_decay)
        )
    )
    final, output_list = lax.scan(advance, start, inputs)
    return (jnp.moveaxis(output_list, 0, 1).reshape(heads, count * BLOCK, -1), final)


def compose(earlier, later):
    return (
        jnp.einsum("hij,hjk->hik", later[0], earlier[0], precision=highest_precision),
        jnp.einsum("hij,hjk->hik", later[0], earlier[1], precision=highest_precision) + later[1],
    )


def slot_places(routes, groups, capacity, experts):
    rows, picks = routes.shape
    flat = routes.reshape(groups, rows // groups * picks)
    matches = (flat[..., None] == jnp.arange(experts, dtype=jnp.int32)).astype(jnp.int32)
    before = jnp.cumsum(matches, axis=1) - matches
    rank = jnp.sum(before * matches, -1)
    group = jnp.arange(groups, dtype=jnp.int32)[:, None]
    return ((flat * groups + group) * capacity + rank).reshape(rows, picks)


def per_device(
    residual_in,
    queries,
    keys,
    values,
    out_gate,
    beta_logit,
    decay_logit,
    decay_log,
    head_gain,
    out_weight,
    norm_gain,
    final_gain,
    expert_index,
    route_weights,
    expert_gate,
    expert_up,
    expert_down,
):
    length, width = residual_in.shape
    heads = beta_logit.shape[0]

    def split_heads(data):
        return data.astype(jnp.float32).reshape(length, heads, HEAD_FEATURES).transpose(1, 0, 2)

    query = unit_rows(split_heads(queries)) * HEAD_FEATURES ** (-0.5)
    key = unit_rows(split_heads(keys))
    value = split_heads(values)
    beta = jax.nn.sigmoid(beta_logit.astype(jnp.float32))
    decay = -jnp.exp(decay_log)[:, None] * jax.nn.softplus(decay_logit.astype(jnp.float32))
    terms = block_terms(query, key, beta, decay)
    identity_map = jnp.broadcast_to(
        jnp.eye(HEAD_FEATURES, dtype=jnp.float32), (heads, HEAD_FEATURES, HEAD_FEATURES)
    )
    blank = jnp.zeros((heads, HEAD_FEATURES, HEAD_FEATURES), jnp.float32)
    extended = jnp.concatenate([blank, identity_map], -1)
    output_list, final = run_blocks(terms, value, extended)
    prefix = carried_in(
        (final[..., HEAD_FEATURES:], final[..., :HEAD_FEATURES]),
        "sp",
        compose,
        (identity_map, blank),
    )
    entry_value = prefix[1]
    mixed = output_list[..., :HEAD_FEATURES] + jnp.einsum(
        "apj,ajz->apz", output_list[..., HEAD_FEATURES:], entry_value, precision=highest_precision
    )
    normalized = mixed * lax.rsqrt(jnp.mean(mixed * mixed, -1, keepdims=True) + 1e-06) * head_gain
    gated = (
        (normalized * jax.nn.silu(split_heads(out_gate)))
        .transpose(1, 0, 2)
        .reshape(length, heads * HEAD_FEATURES)
        .astype(jnp.bfloat16)
    )
    split_count = lax.axis_size("tp")
    expert_count = lax.axis_size("sp") * expert_gate.shape[0]
    rows = length // split_count
    first = lax.axis_index("tp") * rows
    projected = lax.psum_scatter(
        jnp.dot(gated, out_weight, preferred_element_type=jnp.float32).astype(jnp.bfloat16),
        "tp",
        scatter_dimension=0,
        tiled=True,
    ).astype(jnp.float32)
    residual = lax.dynamic_slice_in_dim(residual_in, first, rows, 0)
    routes = lax.dynamic_slice_in_dim(expert_index, first, rows, 0)
    weights = lax.dynamic_slice_in_dim(route_weights, first, rows, 0)
    groups = 1
    capacity = 2 * TOP * (length // split_count) // expert_count
    hidden_in = layer_norm(
        residual_scale * residual.astype(jnp.float32) + projected, norm_gain
    ).astype(jnp.bfloat16)
    places = slot_places(routes, groups, capacity, expert_count)
    slots = expert_count * groups * capacity
    table = (places[:, :, None] == jnp.arange(slots, dtype=jnp.int32)).astype(jnp.bfloat16)
    send = jnp.einsum(
        "rs,rd->sd", jnp.sum(table, 1), hidden_in, preferred_element_type=jnp.float32
    ).astype(jnp.bfloat16)
    arrived = lax.all_to_all(
        send.reshape(expert_count, groups * capacity, width),
        "sp",
        split_axis=0,
        concat_axis=0,
        tiled=True,
    ).reshape(slots, width)
    gate_matrix, up_matrix, down_matrix = (expert_gate[0], expert_up[0], expert_down[0])
    piece = lax.all_gather(arrived, "tp", axis=0, tiled=True)
    gate = jnp.dot(piece, gate_matrix, preferred_element_type=jnp.float32)
    up = jnp.dot(piece, up_matrix, preferred_element_type=jnp.float32)
    inner = (jax.nn.silu(gate) * up).astype(jnp.bfloat16)
    partial_value = jnp.dot(inner, down_matrix, preferred_element_type=jnp.float32)
    result = lax.psum_scatter(
        partial_value.astype(jnp.bfloat16), "tp", scatter_dimension=0, tiled=True
    )
    back = lax.all_to_all(
        result.reshape(expert_count, groups * capacity, width),
        "sp",
        split_axis=0,
        concat_axis=0,
        tiled=True,
    ).reshape(slots, width)
    gathered = jnp.einsum("rks,sd->rkd", table, back, preferred_element_type=jnp.float32)
    routed = jnp.sum(weights[..., None] * gathered, 1)
    layer_out = layer_norm(
        residual_scale * hidden_in.astype(jnp.float32) + routed, final_gain
    ).astype(jnp.bfloat16)
    layer_out = lax.all_gather(layer_out, "tp", axis=0, tiled=True)
    return layer_out


def mm(a, b):
    return jnp.dot(a.astype(jnp.bfloat16), b.astype(jnp.bfloat16), preferred_element_type=jnp.float32)


def mm_nt(a, b):
    return lax.dot_general(
        a.astype(jnp.bfloat16),
        b.astype(jnp.bfloat16),
        (((1,), (1,)), ((), ())),
        preferred_element_type=jnp.float32,
    )


def mm_tn(a, b):
    return lax.dot_general(
        a.astype(jnp.bfloat16),
        b.astype(jnp.bfloat16),
        (((0,), (0,)), ((), ())),
        preferred_element_type=jnp.float32,
    )


scope = jax.named_scope


def pick(table, home):
    chosen = []
    for i in range(len(table[0])):
        value = 0
        for h, order in enumerate(table):
            value = value + (home == h).astype(jnp.int32) * order[i]
        chosen.append(value)
    return chosen


def drain(ref, sem):
    pltpu.make_async_copy(ref, ref, sem).wait()


def layer_kernel(
    n_sp,
    n_tp,
    residual_hbm,
    query_hbm,
    key_hbm,
    value_hbm,
    out_gate_hbm,
    beta_hbm,
    decay_hbm,
    decay_log_hbm,
    head_gain_hbm,
    norm_gain_hbm,
    final_gain_hbm,
    index_hbm,
    weights_hbm,
    out_weight_hbm,
    gate_hbm,
    up_hbm,
    down_hbm,
    out_ref,
    residual_ref,
    query_ref,
    key_ref,
    value_ref,
    out_gate_ref,
    beta_ref,
    decay_ref,
    decay_log_ref,
    head_gain_ref,
    norm_gain_ref,
    final_gain_ref,
    index_ref,
    weights_ref,
    out_weight_v,
    gate_v,
    up_v,
    down_v,
    maps_v,
    adds_v,
    state_in,
    state_out,
    mate_out,
    mate_in,
    entry_v,
    mixed_v,
    readout_v,
    gated_v,
    proj_v,
    proj_in,
    hidden_v,
    send_v,
    arrived_v,
    inner_v,
    own_inner_v,
    part_v,
    part_in,
    pair_v,
    result_v,
    back_v,
    final_v,
    local_sem,
    sent_sem,
    state_sem,
    mate_sem,
    entry_sem,
    proj_sem,
    arrive_sem,
    near_sem,
    full_sem,
    pair_sem,
    part_sem,
    back_sem,
    out_sem,
):
    s = lax.axis_index("sp")
    t = lax.axis_index("tp")
    length, width = residual_ref.shape
    heads = beta_ref.shape[0]
    rows = length // n_tp
    chunks, _, group, cap, _ = arrived_v.shape
    half = width // 2
    right, left = slice(half, width), slice(0, half)
    slots = n_sp * cap
    feat = HEAD_FEATURES
    hidden_units = gate_v.shape[1]

    barrier = pltpu.get_barrier_semaphore()
    for k in range(1, n_sp):
        pl.semaphore_signal(
            barrier, inc=1, device_id=(lax.rem(s + k, n_sp), t), device_id_type=MESH
        )
    for k in range(1, n_tp):
        pl.semaphore_signal(
            barrier, inc=1, device_id=(s, lax.rem(t + k, n_tp)), device_id_type=MESH
        )

    pairs = [
        (decay_hbm, decay_ref),
        (decay_log_hbm, decay_log_ref),
        (beta_hbm, beta_ref),
        (key_hbm, key_ref),
        (query_hbm, query_ref),
        (value_hbm, value_ref),
        (out_gate_hbm, out_gate_ref),
        (head_gain_hbm, head_gain_ref),
        (out_weight_hbm, out_weight_v),
        (index_hbm, index_ref),
        (weights_hbm, weights_ref),
        (residual_hbm, residual_ref),
        (norm_gain_hbm, norm_gain_ref),
        (final_gain_hbm, final_gain_ref),
        (gate_hbm.at[0], gate_v),
        (up_hbm.at[0], up_v),
        (down_hbm.at[0], down_v),
    ]
    local = [pltpu.make_async_copy(a, b, local_sem.at[i]) for i, (a, b) in enumerate(pairs)]
    for copy in local:
        copy.start()

    def remote(src, dst, sem_a, sem_b, to_s, to_t):
        return pltpu.make_async_remote_copy(
            src_ref=src,
            dst_ref=dst,
            send_sem=sem_a,
            recv_sem=sem_b,
            device_id=(to_s, to_t),
            device_id_type=MESH,
        )

    with scope("a_load"):
        for copy in local[:6]:
            copy.wait()
    row_id = lax.broadcasted_iota(jnp.int32, (length, length), 0)
    col_id = lax.broadcasted_iota(jnp.int32, (length, length), 1)
    causal = row_id >= col_id
    strict = row_id > col_id
    eye = (row_id == col_id).astype(jnp.float32)
    tril = causal.astype(jnp.float32)
    beta = jax.nn.sigmoid(beta_ref[...].astype(jnp.float32))
    logit = decay_ref[...].astype(jnp.float32)
    soft = jnp.maximum(logit, 0.0) + jnp.log(1.0 + jnp.exp(-jnp.abs(logit)))
    head_eye = lax.broadcasted_iota(jnp.int32, (heads, heads), 0) == lax.broadcasted_iota(
        jnp.int32, (heads, heads), 1
    )
    rate = jnp.sum(jnp.where(head_eye, jnp.exp(decay_log_ref[...]), 0.0), 1, keepdims=True)
    decay = -rate * soft
    exact = functools.partial(
        lax.dot_general, precision=highest_precision, preferred_element_type=jnp.float32
    )
    nt = (((1,), (1,)), ((), ()))
    run_rows = exact(decay, tril, nt)
    run_cols = exact(tril, decay, nt)
    beta_cols = exact(eye, beta, nt)

    lowers, inverses, rights, score_list, q_list, kd_list, last_list = [], [], [], [], [], [], []
    for h in range(heads):
        cols = slice(h * feat, (h + 1) * feat)
        query = unit_rows(query_ref[:, cols].astype(jnp.float32)) * feat ** (-0.5)
        key = unit_rows(key_ref[:, cols].astype(jnp.float32))
        value = value_ref[:, cols].astype(jnp.float32)
        run_c = run_cols[:, h : h + 1]
        run_r = run_rows[h : h + 1, :]
        beta_c = beta_cols[:, h : h + 1]
        last = run_cols[length - 1 : length, h : h + 1]
        within = jnp.where(causal, jnp.exp(jnp.minimum(run_c - run_r, 0.0)), 0.0)
        lowers.append(jnp.where(strict, mm_nt(key, key) * within * beta_c, 0.0))
        score_list.append((mm_nt(query, key) * within).astype(jnp.bfloat16))
        grown = jnp.exp(run_c)
        rights.append(
            jnp.concatenate([value * beta_c, key * (beta_c * grown)], 1).astype(jnp.bfloat16)
        )
        q_list.append(query * grown)
        kd_list.append((key * jnp.exp(last - run_c)).astype(jnp.bfloat16))
        last_list.append(jnp.exp(last))

    def level(size):
        mid = size // 2
        return (row_id // size == col_id // size) & (row_id % size >= mid) & (col_id % size < mid)

    first = level(2)
    inverses = [eye - jnp.where(first, low, 0.0) for low in lowers]
    size = 4
    while size <= length:
        mask = level(size)
        steps = [mm(jnp.where(mask, low, 0.0), inv) for low, inv in zip(lowers, inverses)]
        inverses = [inv - mm(inv, step) for inv, step in zip(inverses, steps)]
        size *= 2
    solved = [mm(inv, right).astype(jnp.bfloat16) for inv, right in zip(inverses, rights)]
    home, core = s // group, s % group
    mate = home * group + (1 - core)
    after = lax.rem(s + group, n_sp)

    def mate_copy(h):
        return remote(
            mate_out.at[h], mate_in.at[h], sent_sem.at[0], mate_sem.at[h], mate, t
        )

    def state_copy(h):
        return remote(
            state_out.at[h], state_in.at[h], sent_sem.at[1], state_sem.at[h], after, t
        )

    def entry_copy(h):
        return remote(
            state_in.at[h], entry_v.at[h], sent_sem.at[2], entry_sem.at[h], mate, t
        )

    for h in range(heads):
        ends = mm_tn(kd_list[h], solved[h])
        adds_v[h] = ends[:, :feat]
        maps = (last_list[h] * eye[:feat, :feat] - ends[:, feat:]).astype(jnp.bfloat16)
        maps_v[h] = maps
        mate_out[h, 0] = maps
        mate_out[h, 1] = ends[:, :feat].astype(jnp.bfloat16)

    with scope("b_barrier"):
        pl.semaphore_wait(barrier, n_sp - 1 + n_tp - 1)

    @pl.when(core == 0)
    def _():
        for h in range(heads):
            mate_copy(h).start()

    for h in range(heads):
        seen = mm(score_list[h], solved[h])
        mixed_v[h] = seen[:, :feat]
        readout_v[h] = (q_list[h] - seen[:, feat:]).astype(jnp.bfloat16)

    @pl.when(core == 1)
    def _():
        for h in range(heads):
            with scope("c_mate"):
                mate_copy(h).wait_recv()

            @pl.when(home == 0)
            def _():
                state_out[h] = (mm(maps_v[h], mate_in[h, 1]) + adds_v[h]).astype(jnp.bfloat16)
                state_copy(h).start()
                entry_v[h] = mate_in[h, 1]

            @pl.when(home > 0)
            def _():
                both = mm(maps_v[h], jnp.concatenate([mate_in[h, 0], mate_in[h, 1]], 1))
                maps_v[h] = both[:, :feat].astype(jnp.bfloat16)
                adds_v[h] = adds_v[h] + both[:, feat:]

        @pl.when(home > 0)
        def _():
            for h in range(heads):
                with scope("c_state"):
                    state_copy(h).wait_recv()

                @pl.when(home < chunks - 1)
                def _():
                    state_out[h] = (mm(maps_v[h], state_in[h]) + adds_v[h]).astype(jnp.bfloat16)
                    state_copy(h).start()

                entry_copy(h).start()

            for h in range(heads):
                entry_v[h] = (
                    mm(mate_in[h, 0], state_in[h]) + mate_in[h, 1].astype(jnp.float32)
                ).astype(jnp.bfloat16)

    @pl.when((core == 0) & (home == 0))
    def _():
        entry_v[...] = jnp.zeros_like(entry_v)

    @pl.when((core == 0) & (home > 0))
    def _():
        for h in range(heads):
            with scope("c_state"):
                entry_copy(h).wait_recv()

    local[6].wait()
    local[7].wait()
    for h in range(heads):
        cols = slice(h * feat, (h + 1) * feat)
        mixed = mixed_v[h] + mm(readout_v[h], entry_v[h])
        normalized = (
            mixed * lax.rsqrt(jnp.mean(mixed * mixed, -1, keepdims=True) + 1e-06) * head_gain_ref[...]
        )
        gate = out_gate_ref[:, cols].astype(jnp.float32)
        gated_v[:, cols] = (normalized * (gate * jax.nn.sigmoid(gate))).astype(jnp.bfloat16)

    local[8].wait()

    def row_block(i):
        return pl.ds(pl.multiple_of(i * rows, rows), rows)

    def project(i, carry):
        cols = pl.ds(pl.multiple_of(i * 512, 512), 512)
        proj_v[:, cols] = jnp.dot(
            gated_v[...], out_weight_v[:, cols], preferred_element_type=jnp.float32
        ).astype(jnp.bfloat16)
        return carry

    for part in range(4):
        steps = width // 512 // 4
        cols = slice(part * width // 4, (part + 1) * width // 4)
        with scope("d_project"):
            lax.fori_loop(part * steps, (part + 1) * steps, project, 0)
        for k in range(1, n_tp):
            to = lax.rem(t + k, n_tp)
            copy = remote(
                proj_v.at[row_block(to), cols],
                proj_in.at[k - 1, :, cols],
                sent_sem.at[3],
                proj_sem.at[0],
                s,
                to,
            )
            copy.start()

    for copy in local[9:14]:
        copy.wait()
    own_row = (
        lax.broadcasted_iota(jnp.int32, (rows, length), 1)
        == lax.broadcasted_iota(jnp.int32, (rows, length), 0) + t * rows
    ).astype(jnp.float32)
    index = exact(own_row, index_ref[...].astype(jnp.float32), nt)
    weights = exact(own_row, weights_ref[...], nt)
    slot_id = lax.broadcasted_iota(jnp.int32, (rows, slots), 1)
    owner = (slot_id // cap).astype(jnp.float32)
    picks = [(index[:, j : j + 1] == owner).astype(jnp.float32) for j in range(TOP)]
    both = functools.reduce(jnp.add, picks)
    earlier = (
        lax.broadcasted_iota(jnp.int32, (rows, rows), 0)
        > lax.broadcasted_iota(jnp.int32, (rows, rows), 1)
    ).astype(jnp.float32)
    rank = mm(earlier, both)
    here = (rank == (slot_id % cap).astype(jnp.float32)).astype(jnp.float32)
    tables = [(pick * here).astype(jnp.bfloat16) for pick in picks]
    table = (both * here).astype(jnp.bfloat16)

    tx = t + 1 - 2 * lax.rem(t, 2)
    ty = lax.rem(t + 2, 4)
    td = lax.rem(tx + 2, 4)

    def send_copy(to):
        return remote(
            send_v.at[to], arrived_v.at[home, t, core], sent_sem.at[4], arrive_sem.at[home], to, t
        )

    order = pick(VISITS, home)
    legs = [(home, core, 1), (home, 1 - core, 1)] + [(c, 0, group) for c in order[:-1]]

    def fan_out(j):
        c, low, count = legs[j]
        if j > 0:
            with scope("g_arrive"):
                drain(arrived_v.at[c, t, pl.ds(low, count)], arrive_sem.at[c])

        def one(cols, sem, to):
            mine = arrived_v.at[c, t, pl.ds(low, count), :, cols]
            remote(mine, mine, sent_sem.at[5], sem, s, to).start()

        one(left, near_sem.at[j, 0], tx)
        one(right, near_sem.at[j, 1], ty)
        one(right, full_sem.at[c], tx)
        one(left, full_sem.at[c], ty)

    def relay(j):
        c, low, count = legs[j]
        for i, (near, cols, to) in enumerate(((tx, left, ty), (ty, right, tx))):
            block = arrived_v.at[c, near, pl.ds(low, count), :, cols]
            with scope("h_fan"):
                drain(block, near_sem.at[j, i])
            remote(block, block, sent_sem.at[5], full_sem.at[c], s, to).start()

    def wait_full(k):
        with scope("j_full"):
            drain(arrived_v.at[order[k], pl.ds(0, 2)], full_sem.at[order[k]])

    projected = proj_v[row_block(t), :].astype(jnp.float32)
    with scope("e_proj"):
        drain(proj_in, proj_sem.at[0])
    for k in range(1, n_tp):
        projected = projected + proj_in[k - 1].astype(jnp.float32)
    residual = residual_ref[row_block(t), :].astype(jnp.float32)
    hidden_in = layer_norm(residual_scale * residual + projected, norm_gain_ref[...]).astype(
        jnp.bfloat16
    )
    hidden_v[...] = hidden_in

    send_v[...] = mm_tn(table, hidden_in).astype(jnp.bfloat16).reshape(n_sp, cap, width)

    for i in range(group):

        @pl.when(s != home * group + i)
        def _():
            send_copy(home * group + i).start()

    for there in pick(SENDS, home):
        for i in range(group):
            send_copy(there * group + i).start()

    arrived_v[home, t, core] = send_v[s]

    def part_copy(kind, j):
        src, to = (
            (part_v.at[j, td, :, left], tx),
            (part_v.at[j, td, :, right], ty),
            (part_v.at[j, tx, :, left], tx),
            (part_v.at[j, ty, :, right], ty),
            (pair_v.at[0, j], ty),
            (pair_v.at[1, j], tx),
        )[kind]
        sem = pair_sem.at[j, kind] if kind < 2 else part_sem.at[j, kind % 2]
        return remote(src, part_in.at[kind, j], sent_sem.at[6], sem, s, to)

    def gate_up(j, part, inner):
        piece = arrived_v[order[j]].reshape(n_tp * group * cap, width)
        steps = hidden_units // 256 // 2

        def step(i, carry):
            cols = pl.ds(pl.multiple_of(i * 256, 256), 256)
            gate = jnp.dot(piece, gate_v[:, cols], preferred_element_type=jnp.float32)
            up = jnp.dot(piece, up_v[:, cols], preferred_element_type=jnp.float32)
            inner[:, cols] = (gate * jax.nn.sigmoid(gate) * up).astype(jnp.bfloat16)
            return carry

        with scope("k_gateup"):
            lax.fori_loop(part * steps, (part + 1) * steps, step, 0)

    def down(j, inner, kinds):
        def step(i, carry):
            cols = pl.ds(pl.multiple_of(i * 512, 512), 512)
            part_v[j, :, :, cols] = (
                jnp.dot(
                    inner[...], down_v[:, cols], preferred_element_type=jnp.float32
                )
                .astype(jnp.bfloat16)
                .reshape(n_tp, group * cap, 512)
            )
            return carry

        steps = half // 512
        for part in range(2):
            with scope("l_down"):
                lax.fori_loop(part * steps, (part + 1) * steps, step, 0)
            for kind in range(part, kinds, 2):
                part_copy(kind, j).start()

    def pair_up(j):
        wide = jnp.float32
        for i, (near, cols) in enumerate(((ty, left), (tx, right))):
            with scope("m_pair"):
                drain(part_in.at[i, j], pair_sem.at[j, i])
            pair_v[i, j] = (
                part_v[j, near, :, cols].astype(wide) + part_in[i, j].astype(wide)
            ).astype(jnp.bfloat16)
            part_copy(4 + i, j).start()

    def finish(j):
        for i, cols in enumerate((left, right)):
            with scope("n_finish"):
                drain(part_in.at[pl.ds(0, 2), j], part_sem.at[j, i])
            near = part_in[2 + i, j].astype(jnp.float32)
            far = part_in[4 + i, j].astype(jnp.float32)
            total = part_v[j, t, :, cols].astype(jnp.float32) + near + far
            result_v[j, :, :, cols] = total.astype(jnp.bfloat16).reshape(group, cap, half)
            for m in range(group):
                p = order[j] * group + m

                @pl.when(s != p)
                def _():
                    remote(
                        result_v.at[j, m, :, cols],
                        back_v.at[s, :, cols],
                        sent_sem.at[7],
                        back_sem.at[0],
                        p,
                        t,
                    ).start()

                @pl.when(s == p)
                def _():
                    back_v[s, :, cols] = result_v[j, m, :, cols]

    fan_out(0)
    fan_out(1)

    @pl.when(home == 0)
    def _():
        relay(0)
        relay(1)

    fan_out(2)

    @pl.when(home > 0)
    def _():
        relay(0)
        relay(1)

    for copy in local[14:]:
        copy.wait()
    relay(2)

    @pl.when(home != 1)
    def _():
        fan_out(3)

    own = chunks - 1

    @pl.when(home != 1)
    def _():
        wait_full(own)
        gate_up(own, 0, own_inner_v)

    wait_full(0)
    gate_up(0, 0, inner_v)

    @pl.when(home != 1)
    def _():
        relay(3)
        fan_out(4)

    @pl.when(home == 1)
    def _():
        fan_out(3)

    gate_up(0, 1, inner_v)
    down(0, inner_v, 4)

    @pl.when(home == 1)
    def _():
        wait_full(own)
        gate_up(own, 0, own_inner_v)
        gate_up(own, 1, own_inner_v)
        relay(3)
        fan_out(4)
        down(own, own_inner_v, 0)

    wait_full(1)
    gate_up(1, 0, inner_v)
    relay(4)
    gate_up(1, 1, inner_v)

    @pl.when(home != 1)
    def _():
        gate_up(own, 1, own_inner_v)

    pair_up(0)
    down(1, inner_v, 4)
    wait_full(2)
    gate_up(2, 0, inner_v)
    gate_up(2, 1, inner_v)
    pair_up(1)
    finish(0)
    down(2, inner_v, 4)

    @pl.when(home == 1)
    def _():
        part_copy(0, own).start()
        part_copy(1, own).start()

    @pl.when(home != 1)
    def _():
        down(own, own_inner_v, 2)

    finish(1)
    pair_up(2)

    part_copy(2, own).start()
    part_copy(3, own).start()
    pair_up(own)
    finish(2)
    finish(own)

    with scope("o_back"):
        drain(back_v.at[pl.ds(0, n_sp - 1)], back_sem.at[0])

    back = back_v[...].reshape(slots, width)
    chosen = mm(jnp.concatenate(tables, 0), back)
    routed = jnp.zeros((rows, width), jnp.float32)
    for j in range(TOP):
        routed = routed + weights[:, j : j + 1] * chosen[j * rows : (j + 1) * rows]
    final_v[...] = layer_norm(
        residual_scale * hidden_v[...].astype(jnp.float32) + routed, final_gain_ref[...]
    ).astype(jnp.bfloat16)

    def out_copy(owner, q, to, sem):
        cols = pl.ds(q * (width // OUT_PARTS), width // OUT_PARTS)
        cells = out_ref.at[row_block(owner), cols]
        source = final_v.at[:, cols] if owner is t else cells
        return remote(source, cells, sent_sem.at[8], out_sem.at[sem], s, to)

    early = OUT_PARTS // 2
    for q in range(OUT_PARTS):
        rest = 2 * early
        out_copy(t, q, tx, q if q < early else rest).start()
        out_copy(t, OUT_PARTS - 1 - q, ty, early + q if q < early else rest).start()
    own_copy = pltpu.make_async_copy(final_v, out_ref.at[row_block(t)], local_sem.at[17])
    own_copy.start()
    piece = final_v.at[:, pl.ds(0, width // OUT_PARTS)]
    with scope("q_out"):
        for q in range(early):
            drain(piece, out_sem.at[q])
            out_copy(tx, q, ty, 2 * early).start()
            drain(piece, out_sem.at[early + q])
            out_copy(ty, OUT_PARTS - 1 - q, tx, 2 * early).start()

    @pl.when(core == 0)
    def _():
        drain(mate_out, sent_sem.at[0])

    @pl.when((core == 1) & (home < chunks - 1))
    def _():
        drain(state_out, sent_sem.at[1])

    @pl.when((core == 1) & (home > 0))
    def _():
        drain(state_in, sent_sem.at[2])

    drain(proj_in, sent_sem.at[3])
    drain(send_v.at[pl.ds(0, n_sp - 1)], sent_sem.at[4])
    drain(arrived_v.at[:, pl.ds(0, 3)], sent_sem.at[5])
    drain(part_in, sent_sem.at[6])
    drain(back_v.at[pl.ds(0, n_sp - 1)], sent_sem.at[7])
    own_copy.wait()
    with scope("r_out"):
        drain(proj_in.at[pl.ds(0, 2)], out_sem.at[OUT_PARTS])
    with scope("s_sends"):
        drain(proj_in, sent_sem.at[8])


def fused(args, n_sp, n_tp, cap):
    (residual_in, queries, keys, values, out_gate, beta_logit, decay_logit, decay_log, head_gain,
     out_weight, norm_gain, final_gain, expert_index, route_weights, expert_gate, expert_up,
     expert_down) = args
    length, width = residual_in.shape
    heads = beta_logit.shape[0]
    rows = length // n_tp
    chunks = n_sp // GROUP
    units = expert_gate.shape[2]
    feat = HEAD_FEATURES
    low, full = jnp.bfloat16, jnp.float32
    hbm = pl.BlockSpec(memory_space=pl.ANY)
    dma = pltpu.SemaphoreType.DMA
    arrays = [
        residual_in, queries, keys, values, out_gate, beta_logit, decay_logit,
        decay_log.reshape(1, heads), head_gain.reshape(1, -1), norm_gain.reshape(1, -1),
        final_gain.reshape(1, -1), expert_index.T, route_weights.T,
    ]
    return pl.pallas_call(
        functools.partial(layer_kernel, n_sp, n_tp),
        out_shape=pltpu.VMEM((length, width), low),
        in_specs=[hbm] * 17,
        out_specs=hbm,
        scratch_shapes=[pltpu.VMEM(a.shape, a.dtype) for a in arrays]
        + [
            pltpu.VMEM(out_weight.shape, low),
            pltpu.VMEM(expert_gate.shape[1:], low),
            pltpu.VMEM(expert_up.shape[1:], low),
            pltpu.VMEM(expert_down.shape[1:], low),
            pltpu.VMEM((heads, feat, feat), low),
            pltpu.VMEM((heads, feat, feat), full),
            pltpu.VMEM((heads, feat, feat), low),
            pltpu.VMEM((heads, feat, feat), low),
            pltpu.VMEM((heads, 2, feat, feat), low),
            pltpu.VMEM((heads, 2, feat, feat), low),
            pltpu.VMEM((heads, feat, feat), low),
            pltpu.VMEM((heads, length, feat), full),
            pltpu.VMEM((heads, length, feat), low),
            pltpu.VMEM((length, heads * feat), low),
            pltpu.VMEM((length, width), low),
            pltpu.VMEM((n_tp - 1, rows, width), low),
            pltpu.VMEM((rows, width), low),
            pltpu.VMEM((n_sp, cap, width), low),
            pltpu.VMEM((chunks, n_tp, GROUP, cap, width), low),
            pltpu.VMEM((n_tp * GROUP * cap, units), low),
            pltpu.VMEM((n_tp * GROUP * cap, units), low),
            pltpu.VMEM((chunks, n_tp, GROUP * cap, width), low),
            pltpu.VMEM((6, chunks, GROUP * cap, width // 2), low),
            pltpu.VMEM((2, chunks, GROUP * cap, width // 2), low),
            pltpu.VMEM((chunks, GROUP, cap, width), low),
            pltpu.VMEM((n_sp, cap, width), low),
            pltpu.VMEM((rows, width), low),
            dma((18,)),
            dma((9,)),
            dma((heads,)),
            dma((heads,)),
            dma((heads,)),
            dma((1,)),
            dma((chunks,)),
            dma((chunks + 1, 2)),
            dma((chunks,)),
            dma((chunks, 2)),
            dma((chunks, 2)),
            dma((1,)),
            dma((OUT_PARTS + 1,)),
        ],
        compiler_params=pltpu.CompilerParams(
            collective_id=0, has_side_effects=True, vmem_limit_bytes=60 * 1024 * 1024
        ),
    )(*arrays, out_weight, expert_gate, expert_up, expert_down)


def any_size(*args):
    n_sp, n_tp = lax.axis_size("sp"), lax.axis_size("tp")
    residual_in, expert_gate = args[0], args[14]
    length, width = residual_in.shape
    experts = n_sp * expert_gate.shape[0]
    cap = 2 * TOP * (length // n_tp) // experts
    fits = (
        expert_gate.shape[0] == 1
        and n_sp == GROUP * len(VISITS)
        and n_tp == 4
        and length == HEAD_FEATURES
        and cap % 16 == 0
        and (length // n_tp) % 16 == 0
        and (n_sp * cap) % 128 == 0
        and width % 2048 == 0
        and width % (128 * OUT_PARTS) == 0
        and expert_gate.shape[2] % 256 == 0
    )
    return fused(args, n_sp, n_tp, cap) if fits else per_device(*args)


def solution(mesh):
    in_specs = (
        P("sp", None),
        P("sp", "tp"),
        P("sp", "tp"),
        P("sp", "tp"),
        P("sp", "tp"),
        P("tp", "sp"),
        P("tp", "sp"),
        P("tp"),
        P(),
        P("tp", None),
        P(),
        P(),
        P("sp", None),
        P("sp", None),
        P("sp", None, "tp"),
        P("sp", None, "tp"),
        P("sp", "tp", None),
    )
    out_specs = P("sp", None)
    return jax.shard_map(
        any_size, mesh=mesh, in_specs=in_specs, out_specs=out_specs, check_vma=False
    )
```
